1024 devices in a mesh: ep: 64 (over z, core), tp: 16 (over y, x).
Axes of the slice: x: 4, y: 4, z: 32, core: 2. Of those that a mesh axis runs over, the one named last changes fastest.
Arguments:
- tokens: bfloat16 [1024, 2048], P('ep'), may hold values from -6 to 6
- old_state: bfloat16 [1024, 256, 2048], P('ep', None, 'tp'), may hold values from -3 to 3
- first_gain: bfloat16 [2048], replicated, may hold values from 0.099609375 to 1.8984375
- query_weight: bfloat16 [2048, 1024], P('tp'), may hold values from -0.125 to 0.125
- key_weight: bfloat16 [2048, 1024], P('tp'), may hold values from -0.125 to 0.125
- value_weight: bfloat16 [2048, 2048], P(None, 'tp'), may hold values from -0.125 to 0.125
- outgate_weight: bfloat16 [2048, 2048], P(None, 'tp'), may hold values from -0.125 to 0.125
- lowrank_weight: bfloat16 [2048, 16], replicated, may hold values from -0.125 to 0.125
- decay_weight: bfloat16 [16, 1024], replicated, may hold values from -20 to 20
- decay_bias: float32 [1024], replicated, may hold values from -40 to 2
- head_gain: bfloat16 [2048], P('tp'), may hold values from 0.099609375 to 1.8984375
- output_weight: bfloat16 [2048, 2048], P('tp'), may hold values from -0.125 to 0.125
- second_gain: bfloat16 [2048], replicated, may hold values from 0.099609375 to 1.8984375
- expert_gate: bfloat16 [64, 2048, 1920], P('ep', None, 'tp'), may hold values from -0.125 to 0.125
- expert_up: bfloat16 [64, 2048, 1920], P('ep', None, 'tp'), may hold values from -0.125 to 0.125
- expert_down: bfloat16 [64, 1920, 2048], P('ep', 'tp'), may hold values from -0.125 to 0.125
- shared_gate: bfloat16 [2048, 1920], P(None, 'tp'), may hold values from -0.125 to 0.125
- shared_up: bfloat16 [2048, 1920], P(None, 'tp'), may hold values from -0.125 to 0.125
- shared_down: bfloat16 [1920, 2048], P('tp'), may hold values from -0.125 to 0.125
- route_ids: int32 [1024, 4], P('ep'), may hold values from 0 to 63, all different within a row; in each aligned block of 16 rows (0 to 15, 16 to 31, ...) at most 2 rows name the same one
- route_weights: float32 [1024, 4], P('ep'), may hold values from 0.1 to 1
Outputs:
- layer_out: bfloat16 [1024, 2048], P('ep', 'tp')
- new_state: bfloat16 [1024, 256, 2048], P('ep', None, 'tp')
The draws below stay inside these ranges and needn't reach their ends.
Inputs may be any that keep to these rules, and one draw needn't show every extreme that they name: `route_ids`: within the rows of one device (aligned blocks of 16 rows) no expert is named more than 2 times, a bound that some block reaches.
All inputs are finite; a program needn't handle non-finite values.
Results may differ from the reference program's by a relative error of at most 0.035.
Values may be sent and summed in bfloat16 or wider, within the bound.
A program may use at most 32 MiB of HBM per device.

```python
import math
import jax
import jax.numpy as jnp
import numpy as np
from jax import lax

D = 2048
HEADS = 4
DK = 256
DV = 512
RANK = 16
FE = 1920
TOPK = 4
SEQ_DEV = 16
QKW = 1024
VW = 2048
FE_DEV = 120
EXPERTS = 64
CAP = 2
SEQS = 1024
N_EP = 64
N_TP = 16


def block_scale(own_key, dims, cuts, least, largest):
    def one(position, parts):
        heights = jax.random.uniform(jax.random.fold_in(jax.random.fold_in(own_key, 6), position), (parts,), jnp.float32, least / len(cuts), largest / len(cuts))
        return jnp.repeat(jnp.exp(heights), dims[position] // parts).reshape((-1,) + (1,) * (len(dims) - position - 1))

    level = one(*cuts[0])
    for cut in cuts[1:]:
        level = level * one(*cut)
    return level


def routed_block(own_key, own, number, rows, amount, top, reach, lean):
    ranking = jax.random.permutation(own_key, amount)
    crowded, ordinary = portions_of(amount, rows * top, reach, lean, True), portions_of(amount, rows * top, reach, lean, False)
    places = jnp.arange(amount)

    def named(tallies, offset_by):
        used = int((tallies > 0).sum())
        fixed = max(1, used // 4)
        shifted = fixed + (places - fixed + offset_by * (used - fixed)) % max(1, amount - fixed)
        return jnp.zeros((amount,), jnp.int32).at[ranking[jnp.where(places < fixed, places, shifted)]].set(jnp.asarray(tallies, jnp.int32))

    tallies = jnp.where(number % 4 == 0, named(crowded, number // 4), named(ordinary, number - number // 4 - 1))
    mixed = jax.random.permutation(jax.random.fold_in(own, 3), amount)
    source_of, receiver = mixed[0:amount // 2 * 2:2], mixed[1:amount // 2 * 2:2]
    room = jnp.minimum(tallies[source_of] - 1, reach - tallies[receiver]) // 2
    room = jnp.where((source_of == ranking[0]) | (receiver == ranking[0]) | (tallies[receiver] == 0), 0, jnp.maximum(room, 0))
    shifted = jax.random.randint(jax.random.fold_in(own, 4), (amount // 2,), 0, 1 << 20) % (room + 1)
    tallies = tallies.at[source_of].add(-shifted).at[receiver].add(shifted)
    members = jnp.searchsorted(jnp.cumsum(tallies), jnp.arange(rows * top), side="right").astype(jnp.int32)
    table = members.reshape(top, rows).T
    table = table[jax.random.permutation(jax.random.fold_in(own, 1), rows)]
    offset_by = jax.random.randint(jax.random.fold_in(own, 2), (rows, 1), 0, top)
    return jnp.take_along_axis(table, (jnp.arange(top)[None, :] + offset_by) % top, axis=1)


def portions_of(number_of, total, reach, skew, full):
    weights = [(1 << 20) // math.isqrt(standing ** skew) + 1 for standing in range(1, number_of + 1)]
    largest = reach if full else min(reach, max(-(-total // number_of), total * weights[0] // sum(weights)))
    least = 1 if total - largest >= number_of - 1 else 0
    holding, surplus = [largest] + [least] * (number_of - 1), total - largest - least * (number_of - 1)
    while surplus > 0:
        free = [i for i in range(1, number_of) if holding[i] < largest] or [i for i in range(1, number_of) if holding[i] < reach]
        mass, remaining = sum([weights[i] for i in free]), surplus
        for i in free:
            more = min(reach - holding[i], max(1, remaining * weights[i] // mass), surplus)
            holding[i] = holding[i] + more
            surplus = surplus - more
    return np.array(holding)


def centred(stream_key, shape, spread, limit, cuts=(), kind=jnp.bfloat16):
    drawn = jax.random.normal(stream_key, shape, jnp.float32) * spread
    if len(cuts) > 0:
        drawn = block_scale(stream_key, shape, cuts, -0.22, 0.18) * drawn
    return jnp.clip(drawn, min=-limit, max=limit).astype(kind)


def setup_inputs(seed: int = 0) -> dict:
    key_of = jax.random.split(jax.random.key(seed), 22)
    tokens = centred(key_of[0], (SEQS, D), 1.0, 6.0, ((0, 64),))
    old_state = centred(key_of[1], (SEQS, DK, VW), 0.5, 3.0, ((0, 64), (2, 16)))
    first_gain = jnp.clip(1.0 + 0.18 * jax.random.normal(key_of[2], (D,), jnp.float32), 0.099609375, 1.8984375).astype(jnp.bfloat16)
    query_weight = centred(key_of[3], (D, QKW), D ** -0.5, 0.125, ((0, 16),))
    key_weight = centred(key_of[4], (D, QKW), D ** -0.5, 0.125, ((0, 16),))
    value_weight = centred(key_of[5], (D, VW), D ** -0.5, 0.125, ((1, 16),))
    outgate_weight = centred(key_of[6], (D, VW), D ** -0.5, 0.125, ((1, 16),))
    lowrank_weight = centred(key_of[7], (D, RANK), D ** -0.5, 0.125)
    decay_weight = centred(key_of[8], (RANK, QKW), 4.0, 20.0)
    decay_bias = jnp.clip(jax.random.uniform(key_of[9], (QKW,), jnp.float32, -40.0, 2.0), -40.0, 2.0)
    head_gain = jnp.clip(1.0 + 0.18 * jax.random.normal(key_of[10], (VW,), jnp.float32), 0.099609375, 1.8984375).astype(jnp.bfloat16)
    output_weight = centred(key_of[11], (VW, D), VW ** -0.5, 0.125, ((0, 16),))
    second_gain = jnp.clip(1.0 + 0.18 * jax.random.normal(key_of[12], (D,), jnp.float32), 0.099609375, 1.8984375).astype(jnp.bfloat16)
    expert_gate = centred(key_of[13], (EXPERTS, D, FE), D ** -0.5, 0.125, ((0, 64), (2, 16)))
    expert_up = centred(key_of[14], (EXPERTS, D, FE), D ** -0.5, 0.125, ((0, 64), (2, 16)))
    expert_down = centred(key_of[15], (EXPERTS, FE, D), FE ** -0.5, 0.125, ((0, 64), (1, 16)))
    shared_gate = centred(key_of[16], (D, FE), D ** -0.5, 0.125, ((1, 16),))
    shared_up = centred(key_of[17], (D, FE), D ** -0.5, 0.125, ((1, 16),))
    shared_down = centred(key_of[18], (FE, D), FE ** -0.5, 0.125, ((0, 16),))
    route_ids_keys = jax.random.split(jax.random.fold_in(key_of[19], 1), SEQS // SEQ_DEV)
    route_ids_turns = jax.random.permutation(jax.random.fold_in(key_of[19], 3), SEQS // SEQ_DEV)
    route_ids = jax.vmap(lambda own, number: routed_block(jax.random.fold_in(key_of[19], 2), own, number, SEQ_DEV, EXPERTS, TOPK, CAP, 2))(route_ids_keys, route_ids_turns).reshape((SEQS, TOPK))
    route_weights = jnp.clip(jnp.exp(math.log(1.0) - 2.3025851 * jax.random.uniform(key_of[20], (SEQS, TOPK), jnp.float32) ** block_scale(key_of[20], (SEQS, TOPK), ((0, 64),), -0.2, 0.2)), 0.1, 1.0)
    return dict(tokens=tokens, old_state=old_state, first_gain=first_gain, query_weight=query_weight, key_weight=key_weight, value_weight=value_weight, outgate_weight=outgate_weight, lowrank_weight=lowrank_weight, decay_weight=decay_weight, decay_bias=decay_bias, head_gain=head_gain, output_weight=output_weight, second_gain=second_gain, expert_gate=expert_gate, expert_up=expert_up, expert_down=expert_down, shared_gate=shared_gate, shared_up=shared_up, shared_down=shared_down, route_ids=route_ids, route_weights=route_weights)


EPSILON = 1e-06

def rms_norm(values, norm_gain):
    floats = values.astype(jnp.float32)
    scaled = floats * lax.rsqrt(lax.optimization_barrier(jnp.mean(floats * floats, axis=-1, keepdims=True)) + EPSILON)
    return (scaled * norm_gain.astype(jnp.float32)).astype(jnp.bfloat16)

def project(left_side, right_side):
    return jnp.dot(left_side, right_side, preferred_element_type=jnp.float32)

def rounded_blocks(hidden, down_matrix):
    row_count = hidden.shape[0]
    pieces = jnp.einsum('rnf,nfd->nrd', hidden.reshape(row_count, N_TP, FE_DEV).astype(jnp.float32), down_matrix.reshape(N_TP, FE_DEV, D).astype(jnp.float32), precision=lax.Precision.HIGHEST)
    pieces = lax.optimization_barrier(pieces.astype(jnp.bfloat16)).astype(jnp.float32)
    return lax.optimization_barrier(jnp.sum(pieces, axis=0))

def reference(tokens, old_state, first_gain, query_weight, key_weight, value_weight, outgate_weight, lowrank_weight, decay_weight, decay_bias, head_gain, output_weight, second_gain, expert_gate, expert_up, expert_down, shared_gate, shared_up, shared_down, route_ids, route_weights):
    seq_count = tokens.shape[0]
    normed = rms_norm(tokens, first_gain)
    query_rows = project(normed, query_weight).astype(jnp.bfloat16)
    key_rows = project(normed, key_weight).astype(jnp.bfloat16)
    value_rows = project(normed, value_weight).astype(jnp.bfloat16)
    out_gate = project(normed, outgate_weight).astype(jnp.bfloat16)
    lowrank = project(normed, lowrank_weight).astype(jnp.bfloat16)
    log_decay = jax.nn.log_sigmoid(project(lowrank, decay_weight) + decay_bias.astype(jnp.float32)) / 16.0
    decay_rows = jnp.exp(log_decay).reshape(seq_count, HEADS, DK).transpose(0, 2, 1)
    key_cols = key_rows.astype(jnp.float32).reshape(seq_count, HEADS, DK).transpose(0, 2, 1)
    value_cols = value_rows.astype(jnp.float32).reshape(seq_count, HEADS, DV)
    carried = decay_rows[:, :, :, None] * old_state.astype(jnp.float32).reshape(seq_count, DK, HEADS, DV) + key_cols[:, :, :, None] * value_cols[:, None, :, :]
    new_state = carried.reshape(seq_count, DK, VW).astype(jnp.bfloat16)
    query_cols = query_rows.astype(jnp.float32).reshape(seq_count, HEADS, DK)
    read_out = jnp.einsum('bhi,bihc->bhc', query_cols, carried, precision=lax.Precision.HIGHEST) * DK ** (-0.5)
    inverse = lax.rsqrt(lax.optimization_barrier(jnp.mean(read_out * read_out, axis=-1)) + EPSILON)
    mixed_rows = (read_out.reshape(seq_count, VW) * head_gain.astype(jnp.float32) * jax.nn.silu(out_gate.astype(jnp.float32))).astype(jnp.bfloat16)
    per_head = jnp.einsum('bhc,hcd->bhd', mixed_rows.reshape(seq_count, HEADS, DV).astype(jnp.float32), output_weight.reshape(HEADS, DV, D).astype(jnp.float32), precision=lax.Precision.HIGHEST)
    attended = lax.optimization_barrier(jnp.sum(per_head * inverse[:, :, None], axis=1))
    second = (tokens.astype(jnp.float32) + attended).astype(jnp.bfloat16)
    normed_two = rms_norm(second, second_gain)
    shared_hidden = (jax.nn.silu(project(normed_two, shared_gate)) * project(normed_two, shared_up)).astype(jnp.bfloat16)
    shared = rounded_blocks(shared_hidden, shared_down)
    group_ids = route_ids.reshape(N_EP, SEQ_DEV * TOPK).astype(jnp.int32)
    onehot = (group_ids[:, :, None] == jnp.arange(EXPERTS, dtype=jnp.int32)[None, None, :]).astype(jnp.int32)
    slot_rank = lax.optimization_barrier(jnp.sum((jnp.cumsum(onehot, axis=1).astype(jnp.int32) - onehot) * onehot, axis=2)).astype(jnp.int32)
    column = (jnp.arange(N_EP, dtype=jnp.int32)[:, None] * CAP + slot_rank).reshape(-1).astype(jnp.int32)
    flat_ids = group_ids.reshape(-1)
    sources = jnp.repeat(normed_two, TOPK, axis=0)
    buffer = jnp.zeros((EXPERTS, N_EP * CAP, D), jnp.bfloat16).at[flat_ids, column].set(sources)

    def expert_fn(operands):
        incoming, gate_matrix, up_matrix, down_matrix = operands
        hidden = (jax.nn.silu(project(incoming, gate_matrix)) * project(incoming, up_matrix)).astype(jnp.bfloat16)
        return rounded_blocks(hidden, down_matrix).astype(jnp.bfloat16)
    results = lax.map(expert_fn, (buffer, expert_gate, expert_up, expert_down))
    picked = results[flat_ids, column].astype(jnp.float32).reshape(seq_count, TOPK, D)
    routed = lax.optimization_barrier(jnp.sum(picked * route_weights.astype(jnp.float32)[:, :, None], axis=1))
    layer_out = (second.astype(jnp.float32) + shared + routed).astype(jnp.bfloat16)
    return (layer_out, new_state)
```

```python
import functools

import jax
import jax.numpy as jnp
from jax import lax
from jax.experimental import pallas as pl
from jax.experimental.pallas import tpu as pltpu
from jax.sharding import PartitionSpec as P

EPSILON = 1e-06
LANES = 128
CHUNKS = 4
MESH = pl.DeviceIdType.MESH
F32 = jnp.float32
BF16 = jnp.bfloat16


def dot(left, right):
    return jnp.dot(left, right, preferred_element_type=F32)


def dot_t(left, right):
    return lax.dot_general(left, right, (((1,), (1,)), ((), ())), preferred_element_type=F32)


def silu(x):
    return x / (1.0 + jnp.exp(-x))


def kernel(
    sizes,
    tokens_h, state_h, gain1_h, wq_h, wk_h, wv_h, wo_h, wl_h, wd_h, bias_h, hgain_h, wout_h, gain2_h,
    eg_h, eu_h, ed_h, sg_h, su_h, sd_h, ids_h, rw_h,
    out_h, newstate_h,
    tokens, state, gain1, wq, wk, wv, wo, wl, wd, bias, hgain, wout, gain2, eg, eu, ed, sg, su, sd, ids, rw,
    normed, own_normed, a_send, a_recv, b_send, b_recv, c_send, c_recv, n2, s_send, s_recv,
    d_send, d_recv, e_send, e_recv, xn, g_send, g_recv, h_send, h_recv, newstate, out,
    in_sem, out_sem, a_sem, b_sem, c_sem, s_sem, d_sem, e_sem, g_sem, h_sem,
):
    n_ep, n_tp, heads, chunks = sizes
    seqs, width = tokens.shape
    dk, vc = state.shape[1], state.shape[2]
    blocks = width // LANES
    per_head = n_tp // heads
    head_width = vc * per_head
    slots = n_ep * 2
    n_chunk = n_ep // chunks
    rows = n_chunk * 2
    p = lax.axis_index("ep")
    t = lax.axis_index("tp")
    head = t // per_head
    own_cols = pl.ds(pl.multiple_of(t * LANES, LANES), LANES)

    def tp_peer(k):
        return lax.rem(t + k, n_tp)

    def offset_of(i):
        odd = lax.rem(i, 2)
        return odd * ((i + 1) // 2) + (1 - odd) * lax.rem(n_ep - i // 2, n_ep)

    def ep_peer(i):
        return lax.rem(p + offset_of(i), n_ep)

    def wait_bytes(region, sem):
        pltpu.make_async_copy(region, region, sem).wait()

    def to_tp(src_of, dst_of, sems):
        def step(k, carry):
            q = tp_peer(k)
            pltpu.make_async_remote_copy(
                src_of(q), dst_of(k), sems.at[0], sems.at[1], device_id=(p, q), device_id_type=MESH
            ).start()
            return carry

        lax.fori_loop(1, n_tp, step, 0)

    pairs = [
        (tokens_h, tokens), (gain1_h, gain1), (wq_h, wq), (wk_h, wk), (wl_h, wl), (wd_h, wd), (bias_h, bias),
        (wv_h, wv), (wo_h, wo), (ids_h, ids), (rw_h, rw), (hgain_h, hgain), (state_h, state), (wout_h, wout),
        (gain2_h, gain2), (sg_h, sg), (su_h, su), (sd_h, sd), (eg_h, eg), (eu_h, eu), (ed_h, ed),
    ]
    loads = {}
    for number, (src, dst) in enumerate(pairs):
        loads[id(dst)] = (src, dst, in_sem.at[number])

    def ready(*refs):
        for ref in refs:
            pltpu.make_async_copy(*loads[id(ref)]).wait()

    barrier = pltpu.get_barrier_semaphore()

    def greet_tp(k, carry):
        pl.semaphore_signal(barrier, inc=1, device_id=(p, tp_peer(k)), device_id_type=MESH)
        return carry

    def greet_ep(i, carry):
        pl.semaphore_signal(barrier, inc=1, device_id=(lax.rem(p + i, n_ep), t), device_id_type=MESH)
        return carry

    lax.fori_loop(1, n_ep, greet_ep, 0)
    lax.fori_loop(1, n_tp, greet_tp, 0)
    for _, dst in pairs:
        pltpu.make_async_copy(*loads[id(dst)]).start()

    ready(tokens)
    ready(gain1)
    squares = jnp.zeros((seqs, LANES), F32)
    for j in range(blocks):
        x = tokens[:, j * LANES : (j + 1) * LANES].astype(F32)
        squares += x * x
    inverse = lax.rsqrt(jnp.sum(squares, axis=1, keepdims=True) / width + EPSILON)
    gains = gain1[...].astype(F32)
    for j in range(blocks):
        x = tokens[:, j * LANES : (j + 1) * LANES].astype(F32)
        normed[:, j * LANES : (j + 1) * LANES] = (x * inverse * gains[j : j + 1, :]).astype(BF16)
    own_normed[...] = normed[:, own_cols]

    ready(wq)
    ready(wk)
    query_part = dot(own_normed[...], wq[...]).astype(BF16)
    key_part = dot(own_normed[...], wk[...]).astype(BF16)
    for h in range(heads):
        a_send[h, :, :dk] = query_part[:, h * dk : (h + 1) * dk]
        a_send[h, :, dk:] = key_part[:, h * dk : (h + 1) * dk]

    pl.semaphore_wait(barrier, n_ep + n_tp - 2)
    to_tp(lambda q: a_send.at[q // per_head], lambda k: a_recv.at[k - 1], a_sem)

    ready(wl)
    ready(wd)
    ready(bias)
    lowrank = dot_t(normed[...], wl[...]).astype(BF16)
    head_cols = pl.ds(pl.multiple_of(head * dk, dk), dk)
    decay_in = dot(lowrank, wd[:, head_cols])
    bias_all = bias[...]
    bias_row = lax.broadcasted_iota(jnp.int32, bias_all.shape, 0)
    bias_cols = [
        jnp.sum(jnp.where(bias_row == head * (dk // LANES) + m, bias_all, 0.0), axis=0, keepdims=True)
        for m in range(dk // LANES)
    ]
    decay_in = decay_in + jnp.concatenate(bias_cols, axis=1)
    log_decay = -(jnp.maximum(-decay_in, 0.0) + jnp.log1p(jnp.exp(-jnp.abs(decay_in)))) / 16.0
    decay = jnp.exp(log_decay)
    ready(wv)
    ready(wo)
    value = dot(normed[...], wv[...]).astype(BF16)
    out_gate = dot(normed[...], wo[...]).astype(BF16)
    ready(hgain)
    gate = hgain[...].astype(F32) * silu(out_gate.astype(F32))

    ready(ids)
    ready(rw)
    row = lax.broadcasted_iota(jnp.int32, (slots, seqs), 0)
    slot = row // 2
    odd = slot % 2
    offset = odd * ((slot + 1) // 2) + (1 - odd) * ((n_ep - slot // 2) % n_ep)
    expert = (p + offset) % n_ep
    route_ids = ids[...]
    route_weights = rw[...]
    named = jnp.zeros((slots, seqs), F32)
    weight = jnp.zeros((slots, seqs), F32)
    for j in range(route_ids.shape[0]):
        hit = route_ids[j : j + 1, :] == expert
        named = named + jnp.where(hit, 1.0, 0.0)
        weight = weight + jnp.where(hit, route_weights[j : j + 1, :], 0.0)
    earlier = (
        lax.broadcasted_iota(jnp.int32, (seqs, seqs), 0) < lax.broadcasted_iota(jnp.int32, (seqs, seqs), 1)
    )
    rank = dot(named.astype(BF16), jnp.where(earlier, 1.0, 0.0).astype(BF16))
    chosen = jnp.where(rank == (row % 2).astype(F32), named, 0.0)
    placing = chosen.astype(BF16)
    weight = jnp.concatenate([weight * chosen, jnp.zeros((slots, LANES - seqs), F32)], axis=1).T[:seqs]
    weight_hi = weight.astype(BF16)
    weight_lo = (weight - weight_hi.astype(F32)).astype(BF16)

    ready(state)
    ready(wout)

    wait_bytes(a_recv, a_sem.at[1])
    total = a_send[head].astype(F32)
    for k in range(n_tp - 1):
        total = total + a_recv[k].astype(F32)
    query = total[:, :dk].astype(BF16)
    key = total[:, dk:].astype(BF16)
    query_f, key_f = query.astype(F32), key.astype(F32)

    decayed = query_f * decay
    decayed_hi = decayed.astype(BF16)
    decayed_lo = (decayed - decayed_hi.astype(F32)).astype(BF16)
    both = jnp.concatenate([decayed_hi, decayed_lo], axis=0)
    row = lax.broadcasted_iota(jnp.int32, (seqs, vc), 0)
    read = jnp.sum(query_f * key_f, axis=1, keepdims=True) * value.astype(F32)
    for b in range(seqs):
        got = dot(both, state[b])
        read = read + jnp.where(row == b, got[:seqs] + got[seqs:], 0.0)
    read = read * dk**-0.5
    own_squares = jnp.sum(read * read, axis=1, keepdims=True)
    mixed = (read * gate).astype(BF16)
    part = dot(mixed, wout[...]).astype(BF16)
    sq_hi = own_squares.astype(BF16).astype(F32)
    sq_lo = (own_squares - sq_hi).astype(BF16).astype(F32)
    first_lanes = lax.broadcasted_iota(jnp.int32, (seqs, LANES), 1)
    carried_squares = jnp.where(first_lanes == 0, sq_hi, jnp.where(first_lanes == 1, sq_lo, 0.0)).astype(BF16)
    for q in range(n_tp):
        b_send[q, :seqs, :] = part[:, q * LANES : (q + 1) * LANES]
        b_send[q, seqs:, :] = carried_squares
    to_tp(lambda q: b_send.at[q], lambda k: b_recv.at[t], b_sem)
    b_recv[t] = b_send[t]

    padded = jnp.concatenate(
        [
            key_f,
            decay.astype(BF16).astype(F32),
            (decay - decay.astype(BF16).astype(F32)),
            jnp.zeros((LANES - 3 * seqs, dk), F32),
        ],
        axis=0,
    )
    columns = padded.T.astype(BF16)
    value_rows = jnp.concatenate([value.astype(F32), jnp.zeros((LANES - seqs, vc), F32)], axis=0)
    wide_row = lax.broadcasted_iota(jnp.int32, (LANES, vc), 0)
    ready(gain2)
    gains = gain2[...].astype(F32)

    wait_bytes(b_recv.at[pl.ds(0, n_tp - 1)], b_sem.at[1])
    second = tokens[:, own_cols].astype(F32)
    for h in range(heads):
        parts = jnp.zeros((seqs, LANES), F32)
        sums = jnp.zeros((seqs, LANES), F32)
        for q in range(h * per_head, (h + 1) * per_head):
            got = b_recv[q].astype(F32)
            parts = parts + got[:seqs]
            sums = sums + got[seqs:]
        scale = lax.rsqrt(jnp.sum(sums, axis=1, keepdims=True) / head_width + EPSILON)
        second = second + scale * parts
    second = second.astype(BF16)
    c_send[...] = second

    d_send[...] = dot(placing, second).reshape(n_ep, 2, LANES).astype(BF16)

    def dispatch(step, carry):
        i = n_ep - 1 - step
        pltpu.make_async_remote_copy(
            d_send.at[i], d_recv.at[i], d_sem.at[0], d_sem.at[1 + i // n_chunk],
            device_id=(ep_peer(i), t), device_id_type=MESH,
        ).start()
        return carry

    lax.fori_loop(0, n_ep - 1, dispatch, 0)
    to_tp(lambda q: c_send, lambda k: c_recv.at[t], c_sem)
    c_recv[t] = second
    d_recv[0] = d_send[0]

    def update(b, carry):
        right = jnp.concatenate(
            [
                jnp.where(wide_row == b, value_rows, 0.0),
                jnp.where((wide_row == seqs + b) | (wide_row == 2 * seqs + b), 1.0, 0.0),
            ],
            axis=1,
        ).astype(BF16)
        made = dot(columns, right)
        newstate[b] = (made[:, vc:] * state[b].astype(F32) + made[:, :vc]).astype(BF16)
        pltpu.make_async_copy(newstate.at[b], newstate_h.at[b], out_sem.at[1]).start()
        return carry

    lax.fori_loop(0, seqs, update, 0)

    def normalise(pieces, result, count):
        squares = jnp.zeros((count, LANES), F32)
        for j in range(blocks):
            x = pieces(j).astype(F32)
            squares = squares + x * x
        inverse = lax.rsqrt(jnp.sum(squares, axis=1, keepdims=True) / width + EPSILON)
        for j in range(blocks):
            x = pieces(j).astype(F32)
            result[:, j * LANES : (j + 1) * LANES] = (x * inverse * gains[j : j + 1, :]).astype(BF16)

    wait_bytes(c_recv.at[pl.ds(0, n_tp - 1)], c_sem.at[1])
    normalise(lambda j: c_recv[j], n2, seqs)
    ready(sg)
    ready(su)
    ready(sd)
    hidden = (silu(dot_t(n2[...], sg[...])) * dot_t(n2[...], su[...])).astype(BF16)
    down = dot(hidden, sd[...]).astype(BF16)
    for q in range(n_tp):
        s_send[q] = down[:, q * LANES : (q + 1) * LANES]
    to_tp(lambda q: s_send.at[q], lambda k: s_recv.at[k - 1], s_sem)
    ready(eg)
    ready(eu)
    ready(ed)

    def gather(c):
        first = 1 if c == 0 else c * n_chunk
        wait_bytes(d_recv.at[pl.ds(first, (c + 1) * n_chunk - first)], d_sem.at[1 + c])
        block = d_recv[c * n_chunk : (c + 1) * n_chunk].astype(F32).reshape(rows, LANES).astype(BF16)
        e_send[c] = block
        to_tp(lambda q: e_send.at[c], lambda k: e_recv.at[c, t], e_sem.at[c])
        e_recv[c, t] = block

    def experts(c):
        wait_bytes(e_recv.at[c, pl.ds(0, n_tp - 1)], e_sem.at[c, 1])
        normalise(lambda j: e_recv[c, j], xn, rows)
        hidden = (silu(dot_t(xn[...], eg[0])) * dot_t(xn[...], eu[0])).astype(BF16)
        down = dot(hidden, ed[0]).astype(BF16)
        for q in range(n_tp):
            g_send[c, q] = down[:, q * LANES : (q + 1) * LANES]
        to_tp(lambda q: g_send.at[c, q], lambda k: g_recv.at[c, k - 1], g_sem.at[c])

    def give_back(c):
        wait_bytes(g_recv.at[c], g_sem.at[c, 1])
        total = g_send[c, t].astype(F32)
        for k in range(n_tp - 1):
            total = total + g_recv[c, k].astype(F32)
        h_send[c * n_chunk : (c + 1) * n_chunk] = total.reshape(n_chunk, 2, LANES).astype(BF16)
        first = 1 if c == 0 else c * n_chunk

        def step(s, carry):
            i = (c + 1) * n_chunk - 1 - s
            back = lax.rem(p + n_ep - offset_of(i), n_ep)
            pltpu.make_async_remote_copy(
                h_send.at[i], h_recv.at[i], h_sem.at[0], h_sem.at[1],
                device_id=(back, t), device_id_type=MESH,
            ).start()
            return carry

        lax.fori_loop(0, (c + 1) * n_chunk - first, step, 0)
        if c == 0:
            h_recv[0] = h_send[0]

    for c in range(chunks):
        gather(c)
        if c >= 1:
            experts(c - 1)
        if c >= 2:
            give_back(c - 2)
    if chunks >= 2:
        give_back(chunks - 2)
    experts(chunks - 1)
    give_back(chunks - 1)

    wait_bytes(s_recv, s_sem.at[1])
    total = s_send[t].astype(F32)
    for k in range(n_tp - 1):
        total = total + s_recv[k].astype(F32)
    total = total + c_send[...].astype(F32)
    wait_bytes(a_recv, a_sem.at[0])
    wait_bytes(b_recv.at[pl.ds(0, n_tp - 1)], b_sem.at[0])
    wait_bytes(c_recv.at[pl.ds(0, n_tp - 1)], c_sem.at[0])
    wait_bytes(s_recv, s_sem.at[0])
    wait_bytes(d_recv.at[pl.ds(1, n_ep - 1)], d_sem.at[0])
    for c in range(chunks):
        wait_bytes(e_recv.at[c, pl.ds(0, n_tp - 1)], e_sem.at[c, 0])
        wait_bytes(g_recv.at[c], g_sem.at[c, 0])
    wait_bytes(newstate, out_sem.at[1])

    wait_bytes(h_recv.at[pl.ds(1, n_ep - 1)], h_sem.at[1])
    returned = h_recv[...].astype(F32).reshape(slots, LANES).astype(BF16)
    total = total + dot(weight_hi, returned) + dot(weight_lo, returned)
    out[...] = total.astype(BF16)
    result = pltpu.make_async_copy(out, out_h, out_sem.at[0])
    result.start()
    wait_bytes(h_recv.at[pl.ds(1, n_ep - 1)], h_sem.at[0])
    result.wait()


def body(n_ep, n_tp, *args):
    (
        tokens, old_state, first_gain, query_weight, key_weight, value_weight, outgate_weight, lowrank_weight,
        decay_weight, decay_bias, head_gain, output_weight, second_gain, expert_gate, expert_up, expert_down,
        shared_gate, shared_up, shared_down, route_ids, route_weights,
    ) = args
    seqs, width = tokens.shape
    dk = old_state.shape[1]
    heads = decay_weight.shape[1] // dk
    chunks = CHUNKS
    blocks = width // LANES
    operands = [
        tokens, old_state, first_gain.reshape(blocks, LANES), query_weight, key_weight, value_weight, outgate_weight,
        lowrank_weight.T, decay_weight, decay_bias.reshape(-1, LANES), head_gain.reshape(1, -1), output_weight,
        second_gain.reshape(blocks, LANES), expert_gate.swapaxes(1, 2), expert_up.swapaxes(1, 2), expert_down,
        shared_gate.T, shared_up.T, shared_down, route_ids.T, route_weights.T,
    ]
    rows = 2 * n_ep // chunks
    vmem = lambda shape, dtype=BF16: pltpu.VMEM(shape, dtype)
    dma = pltpu.SemaphoreType.DMA
    scratch = [vmem(x.shape, x.dtype) for x in operands]
    scratch += [
        vmem((seqs, width)),
        vmem((seqs, LANES)),
        vmem((heads, seqs, 2 * dk)),
        vmem((n_tp - 1, seqs, 2 * dk)),
        vmem((n_tp, 2 * seqs, LANES)),
        vmem((n_tp, 2 * seqs, LANES)),
        vmem((seqs, LANES)),
        vmem((n_tp, seqs, LANES)),
        vmem((seqs, width)),
        vmem((n_tp, seqs, LANES)),
        vmem((n_tp - 1, seqs, LANES)),
        vmem((n_ep, 2, LANES)),
        vmem((n_ep, 2, LANES)),
        vmem((chunks, rows, LANES)),
        vmem((chunks, n_tp, rows, LANES)),
        vmem((rows, width)),
        vmem((chunks, n_tp, rows, LANES)),
        vmem((chunks, n_tp - 1, rows, LANES)),
        vmem((n_ep, 2, LANES)),
        vmem((n_ep, 2, LANES)),
        vmem(old_state.shape),
        vmem((seqs, LANES)),
        dma((len(operands),)),
        dma((2,)),
        dma((2,)),
        dma((2,)),
        dma((2,)),
        dma((2,)),
        dma((1 + chunks,)),
        dma((chunks, 2)),
        dma((chunks, 2)),
        dma((2,)),
    ]
    return pl.pallas_call(
        functools.partial(kernel, (n_ep, n_tp, heads, chunks)),
        out_shape=(
            jax.ShapeDtypeStruct((seqs, LANES), BF16),
            jax.ShapeDtypeStruct(old_state.shape, BF16),
        ),
        in_specs=[pl.BlockSpec(memory_space=pltpu.HBM)] * len(operands),
        out_specs=(pl.BlockSpec(memory_space=pl.ANY), pl.BlockSpec(memory_space=pl.ANY)),
        scratch_shapes=scratch,
        compiler_params=pltpu.CompilerParams(
            collective_id=0, has_side_effects=True
        ),
    )(*operands)


def solution(mesh):
    return jax.shard_map(
        functools.partial(body, mesh.shape["ep"], mesh.shape["tp"]),
        mesh=mesh,
        in_specs=(
            P("ep", None),
            P("ep", None, "tp"),
            P(),
            P("tp", None),
            P("tp", None),
            P(None, "tp"),
            P(None, "tp"),
            P(),
            P(),
            P(),
            P("tp"),
            P("tp", None),
            P(),
            P("ep", None, "tp"),
            P("ep", None, "tp"),
            P("ep", "tp", None),
            P(None, "tp"),
            P(None, "tp"),
            P("tp", None),
            P("ep", None),
            P("ep", None),
        ),
        out_specs=(P("ep", "tp"), P("ep", None, "tp")),
        check_vma=False,
    )
```

```python
import functools

import jax
import jax.numpy as jnp
from jax import lax
from jax.experimental import pallas as pl
from jax.experimental.pallas import tpu as pltpu
from jax.sharding import PartitionSpec as P

EPSILON = 1e-06
LANES = 128
CHUNKS = 4
MESH = pl.DeviceIdType.MESH
F32 = jnp.float32
BF16 = jnp.bfloat16


def dot(left, right):
    return jnp.dot(left, right, preferred_element_type=F32)


def dot_t(left, right):
    return lax.dot_general(left, right, (((1,), (1,)), ((), ())), preferred_element_type=F32)


def silu(x):
    return x / (1.0 + jnp.exp(-x))


def kernel(
    sizes,
    tokens_h, state_h, gain1_h, wq_h, wk_h, wv_h, wo_h, wl_h, wd_h, bias_h, hgain_h, wout_h, gain2_h,
    eg_h, eu_h, ed_h, sg_h, su_h, sd_h, ids_h, rw_h,
    out, newstate,
    tokens, state, gain1, wq, wk, wv, wo, wl, wd, bias, hgain, wout, gain2, eg, eu, ed, sg, su, sd, ids, rw,
    normed, own_normed, a_send, a_recv, b_send, b_recv, c_send, c_recv, n2, s_send, s_recv,
    d_send, d_recv, e_send, e_recv, xn, g_send, g_recv, h_send, h_recv,
    in_sem, a_sem, b_sem, c_sem, s_sem, d_sem, e_sem, g_sem, h_sem, z_sem,
):
    n_ep, n_tp, heads, chunks = sizes
    seqs, width = tokens.shape
    dk, vc = state.shape[1], state.shape[2]
    blocks = width // LANES
    per_head = n_tp // heads
    head_width = vc * per_head
    slots = n_ep * 2
    n_chunk = n_ep // chunks
    rows = n_chunk * 2
    p = lax.axis_index("ep")
    t = lax.axis_index("tp")
    head = t // per_head
    own_cols = pl.ds(pl.multiple_of(t * LANES, LANES), LANES)

    def tp_peer(k):
        return lax.rem(t + k, n_tp)

    def offset_of(i):
        odd = lax.rem(i, 2)
        return odd * ((i + 1) // 2) + (1 - odd) * lax.rem(n_ep - i // 2, n_ep)

    def ep_peer(i):
        return lax.rem(p + offset_of(i), n_ep)

    def wait_bytes(region, sem):
        pltpu.make_async_copy(region, region, sem).wait()

    def to_tp(src_of, dst_of, sems):
        def step(k, carry):
            q = tp_peer(k)
            pltpu.make_async_remote_copy(
                src_of(q), dst_of(k), sems.at[0], sems.at[1], device_id=(p, q), device_id_type=MESH
            ).start()
            return carry

        lax.fori_loop(1, n_tp, step, 0)

    pairs = [
        (tokens_h, tokens), (gain1_h, gain1), (wq_h, wq), (wk_h, wk), (wl_h, wl), (wd_h, wd), (bias_h, bias),
        (wv_h, wv), (wo_h, wo), (ids_h, ids), (rw_h, rw), (hgain_h, hgain), (state_h, state), (wout_h, wout),
        (gain2_h, gain2), (sg_h, sg), (su_h, su), (sd_h, sd), (eg_h, eg), (eu_h, eu), (ed_h, ed),
    ]
    loads = {}
    for number, (src, dst) in enumerate(pairs):
        loads[id(dst)] = (src, dst, in_sem.at[number])

    def ready(*refs):
        for ref in refs:
            pltpu.make_async_copy(*loads[id(ref)]).wait()

    barrier = pltpu.get_barrier_semaphore()
    n_z = n_ep // 2
    z, core = p // 2, lax.rem(p, 2)

    def chip(d):
        return lax.rem(z + n_z + d, n_z)

    def greet_tp(k, carry):
        pl.semaphore_signal(barrier, inc=1, device_id=(p, tp_peer(k)), device_id_type=MESH)
        return carry

    early = (tokens, gain1, wq, wk)
    for ref in early:
        pltpu.make_async_copy(*loads[id(ref)]).start()
    near = [2 * z + 1 - core] + [2 * chip(d) + c for d in (1, -1) for c in (0, 1)]
    for q in near:
        pl.semaphore_signal(barrier, inc=1, device_id=(q, t), device_id_type=MESH)
    lax.fori_loop(1, n_tp, greet_tp, 0)
    for _, dst in pairs:
        if all(dst is not ref for ref in early):
            pltpu.make_async_copy(*loads[id(dst)]).start()

    rounds = []
    while 2 ** len(rounds) < n_z // 2:
        rounds.append(2 ** len(rounds))

    def tell(r):
        if r < len(rounds):
            for d in (rounds[r], -rounds[r]):
                pl.semaphore_signal(z_sem.at[r], inc=1, device_id=(2 * chip(d) + core, t), device_id_type=MESH)

    def hear(r):
        if r < len(rounds):
            pl.semaphore_wait(z_sem.at[r], 2)

    ready(tokens)
    ready(gain1)
    squares = jnp.zeros((seqs, LANES), F32)
    for j in range(blocks):
        x = tokens[:, j * LANES : (j + 1) * LANES].astype(F32)
        squares += x * x
    inverse = lax.rsqrt(jnp.sum(squares, axis=1, keepdims=True) / width + EPSILON)
    gains = gain1[...].astype(F32)
    for j in range(blocks):
        x = tokens[:, j * LANES : (j + 1) * LANES].astype(F32)
        normed[:, j * LANES : (j + 1) * LANES] = (x * inverse * gains[j : j + 1, :]).astype(BF16)
    own_normed[...] = normed[:, own_cols]

    ready(wq)
    ready(wk)
    query_part = dot(own_normed[...], wq[...]).astype(BF16)
    key_part = dot(own_normed[...], wk[...]).astype(BF16)
    for h in range(heads):
        a_send[h, :, :dk] = query_part[:, h * dk : (h + 1) * dk]
        a_send[h, :, dk:] = key_part[:, h * dk : (h + 1) * dk]

    pl.semaphore_wait(barrier, n_tp - 1 + len(near))
    to_tp(lambda q: a_send.at[q // per_head], lambda k: a_recv.at[k - 1], a_sem)
    tell(0)

    ready(wl)
    ready(wd)
    ready(bias)
    lowrank = dot_t(normed[...], wl[...]).astype(BF16)
    head_cols = pl.ds(pl.multiple_of(head * dk, dk), dk)
    decay_in = dot(lowrank, wd[:, head_cols])
    bias_all = bias[...]
    bias_row = lax.broadcasted_iota(jnp.int32, bias_all.shape, 0)
    bias_cols = [
        jnp.sum(jnp.where(bias_row == head * (dk // LANES) + m, bias_all, 0.0), axis=0, keepdims=True)
        for m in range(dk // LANES)
    ]
    decay_in = decay_in + jnp.concatenate(bias_cols, axis=1)
    log_decay = -(jnp.maximum(-decay_in, 0.0) + jnp.log1p(jnp.exp(-jnp.abs(decay_in)))) / 16.0
    decay = jnp.exp(log_decay)
    ready(wv)
    ready(wo)
    value = dot(normed[...], wv[...]).astype(BF16)
    out_gate = dot(normed[...], wo[...]).astype(BF16)
    ready(hgain)
    gate = hgain[...].astype(F32) * silu(out_gate.astype(F32))

    ready(ids)
    ready(rw)
    row = lax.broadcasted_iota(jnp.int32, (slots, seqs), 0)
    slot = row // 2
    odd = slot % 2
    offset = odd * ((slot + 1) // 2) + (1 - odd) * ((n_ep - slot // 2) % n_ep)
    expert = (p + offset) % n_ep
    route_ids = ids[...]
    route_weights = rw[...]
    named = jnp.zeros((slots, seqs), F32)
    weight = jnp.zeros((slots, seqs), F32)
    for j in range(route_ids.shape[0]):
        hit = route_ids[j : j + 1, :] == expert
        named = named + jnp.where(hit, 1.0, 0.0)
        weight = weight + jnp.where(hit, route_weights[j : j + 1, :], 0.0)
    earlier = (
        lax.broadcasted_iota(jnp.int32, (seqs, seqs), 0) < lax.broadcasted_iota(jnp.int32, (seqs, seqs), 1)
    )
    rank = dot(named.astype(BF16), jnp.where(earlier, 1.0, 0.0).astype(BF16))
    chosen = jnp.where(rank == (row % 2).astype(F32), named, 0.0)
    placing = chosen.astype(BF16)
    weight = jnp.concatenate([weight * chosen, jnp.zeros((slots, LANES - seqs), F32)], axis=1).T[:seqs]
    weight_hi = weight.astype(BF16)
    weight_lo = (weight - weight_hi.astype(F32)).astype(BF16)

    ready(state)
    ready(wout)

    hear(0)
    tell(1)
    hear(1)
    tell(2)

    wait_bytes(a_recv, a_sem.at[1])
    hear(2)
    tell(3)
    total = a_send[head].astype(F32)
    for k in range(n_tp - 1):
        total = total + a_recv[k].astype(F32)
    query = total[:, :dk].astype(BF16)
    key = total[:, dk:].astype(BF16)
    query_f, key_f = query.astype(F32), key.astype(F32)

    decayed = query_f * decay
    decayed_hi = decayed.astype(BF16)
    decayed_lo = (decayed - decayed_hi.astype(F32)).astype(BF16)
    both = jnp.concatenate([decayed_hi, decayed_lo], axis=0)
    row = lax.broadcasted_iota(jnp.int32, (seqs, vc), 0)
    read = jnp.sum(query_f * key_f, axis=1, keepdims=True) * value.astype(F32)
    for b in range(seqs):
        got = dot(both, state[b])
        read = read + jnp.where(row == b, got[:seqs] + got[seqs:], 0.0)
    read = read * dk**-0.5
    own_squares = jnp.sum(read * read, axis=1, keepdims=True)
    mixed = (read * gate).astype(BF16)
    part = dot(mixed, wout[...]).astype(BF16)
    sq_hi = own_squares.astype(BF16).astype(F32)
    sq_lo = (own_squares - sq_hi).astype(BF16).astype(F32)
    first_lanes = lax.broadcasted_iota(jnp.int32, (seqs, LANES), 1)
    carried_squares = jnp.where(first_lanes == 0, sq_hi, jnp.where(first_lanes == 1, sq_lo, 0.0)).astype(BF16)
    for q in range(n_tp):
        b_send[q, :seqs, :] = part[:, q * LANES : (q + 1) * LANES]
        b_send[q, seqs:, :] = carried_squares
    to_tp(lambda q: b_send.at[q], lambda k: b_recv.at[t], b_sem)
    b_recv[t] = b_send[t]

    padded = jnp.concatenate(
        [
            key_f,
            decay.astype(BF16).astype(F32),
            (decay - decay.astype(BF16).astype(F32)),
            jnp.zeros((LANES - 3 * seqs, dk), F32),
        ],
        axis=0,
    )
    columns = padded.T.astype(BF16)
    value_rows = jnp.concatenate([value.astype(F32), jnp.zeros((LANES - seqs, vc), F32)], axis=0)
    wide_row = lax.broadcasted_iota(jnp.int32, (LANES, vc), 0)
    ready(gain2)
    gains = gain2[...].astype(F32)

    def update(b, carry):
        right = jnp.concatenate(
            [
                jnp.where(wide_row == b, value_rows, 0.0),
                jnp.where((wide_row == seqs + b) | (wide_row == 2 * seqs + b), 1.0, 0.0),
            ],
            axis=1,
        ).astype(BF16)
        made = dot(columns, right)
        newstate[b] = (made[:, vc:] * state[b].astype(F32) + made[:, :vc]).astype(BF16)
        return carry

    lax.fori_loop(0, seqs, update, 0)

    wait_bytes(b_recv.at[pl.ds(0, n_tp - 1)], b_sem.at[1])
    second = tokens[:, own_cols].astype(F32)
    for h in range(heads):
        parts = jnp.zeros((seqs, LANES), F32)
        sums = jnp.zeros((seqs, LANES), F32)
        for q in range(h * per_head, (h + 1) * per_head):
            got = b_recv[q].astype(F32)
            parts = parts + got[:seqs]
            sums = sums + got[seqs:]
        scale = lax.rsqrt(jnp.sum(sums, axis=1, keepdims=True) / head_width + EPSILON)
        second = second + scale * parts
    second = second.astype(BF16)
    c_send[...] = second

    d_send[...] = dot(placing, second).reshape(n_ep, 2, LANES).astype(BF16)

    hear(3)

    def dispatch(step, carry):
        i = n_ep - 1 - step
        pltpu.make_async_remote_copy(
            d_send.at[i], d_recv.at[i], d_sem.at[0], d_sem.at[1 + i // n_chunk],
            device_id=(ep_peer(i), t), device_id_type=MESH,
        ).start()
        return carry

    lax.fori_loop(0, n_ep - 1, dispatch, 0)
    to_tp(lambda q: c_send, lambda k: c_recv.at[t], c_sem)
    c_recv[t] = second
    d_recv[0] = d_send[0]

    def normalise(pieces, result, count):
        squares = jnp.zeros((count, LANES), F32)
        for j in range(blocks):
            x = pieces(j).astype(F32)
            squares = squares + x * x
        inverse = lax.rsqrt(jnp.sum(squares, axis=1, keepdims=True) / width + EPSILON)
        for j in range(blocks):
            x = pieces(j).astype(F32)
            result[:, j * LANES : (j + 1) * LANES] = (x * inverse * gains[j : j + 1, :]).astype(BF16)

    wait_bytes(c_recv.at[pl.ds(0, n_tp - 1)], c_sem.at[1])
    normalise(lambda j: c_recv[j], n2, seqs)
    ready(sg)
    ready(su)
    ready(sd)
    hidden = (silu(dot_t(n2[...], sg[...])) * dot_t(n2[...], su[...])).astype(BF16)
    down = dot(hidden, sd[...]).astype(BF16)
    for q in range(n_tp):
        s_send[q] = down[:, q * LANES : (q + 1) * LANES]
    to_tp(lambda q: s_send.at[q], lambda k: s_recv.at[k - 1], s_sem)
    ready(eg)
    ready(eu)
    ready(ed)

    def gather(c):
        first = 1 if c == 0 else c * n_chunk
        wait_bytes(d_recv.at[pl.ds(first, (c + 1) * n_chunk - first)], d_sem.at[1 + c])
        block = d_recv[c * n_chunk : (c + 1) * n_chunk].astype(F32).reshape(rows, LANES).astype(BF16)
        e_send[c] = block
        to_tp(lambda q: e_send.at[c], lambda k: e_recv.at[c, t], e_sem.at[c])
        e_recv[c, t] = block

    def experts(c):
        wait_bytes(e_recv.at[c, pl.ds(0, n_tp - 1)], e_sem.at[c, 1])
        normalise(lambda j: e_recv[c, j], xn, rows)
        hidden = (silu(dot_t(xn[...], eg[0])) * dot_t(xn[...], eu[0])).astype(BF16)
        down = dot(hidden, ed[0]).astype(BF16)
        for q in range(n_tp):
            g_send[c, q] = down[:, q * LANES : (q + 1) * LANES]
        to_tp(lambda q: g_send.at[c, q], lambda k: g_recv.at[c, k - 1], g_sem.at[c])

    def give_back(c):
        wait_bytes(g_recv.at[c], g_sem.at[c, 1])
        total = g_send[c, t].astype(F32)
        for k in range(n_tp - 1):
            total = total + g_recv[c, k].astype(F32)
        h_send[c * n_chunk : (c + 1) * n_chunk] = total.reshape(n_chunk, 2, LANES).astype(BF16)
        first = 1 if c == 0 else c * n_chunk

        def step(s, carry):
            i = (c + 1) * n_chunk - 1 - s
            back = lax.rem(p + n_ep - offset_of(i), n_ep)
            pltpu.make_async_remote_copy(
                h_send.at[i], h_recv.at[i], h_sem.at[0], h_sem.at[1],
                device_id=(back, t), device_id_type=MESH,
            ).start()
            return carry

        lax.fori_loop(0, (c + 1) * n_chunk - first, step, 0)
        if c == 0:
            h_recv[0] = h_send[0]

    for c in range(chunks):
        gather(c)
        if c >= 1:
            experts(c - 1)
    experts(chunks - 1)
    for c in range(chunks):
        give_back(c)

    wait_bytes(s_recv, s_sem.at[1])
    total = s_send[t].astype(F32)
    for k in range(n_tp - 1):
        total = total + s_recv[k].astype(F32)
    total = total + c_send[...].astype(F32)
    wait_bytes(a_recv, a_sem.at[0])
    wait_bytes(b_recv.at[pl.ds(0, n_tp - 1)], b_sem.at[0])
    wait_bytes(c_recv.at[pl.ds(0, n_tp - 1)], c_sem.at[0])
    wait_bytes(s_recv, s_sem.at[0])
    wait_bytes(d_recv.at[pl.ds(1, n_ep - 1)], d_sem.at[0])
    for c in range(chunks):
        wait_bytes(e_recv.at[c, pl.ds(0, n_tp - 1)], e_sem.at[c, 0])
        wait_bytes(g_recv.at[c], g_sem.at[c, 0])

    wait_bytes(h_recv.at[pl.ds(1, n_ep - 1)], h_sem.at[1])
    returned = h_recv[...].astype(F32).reshape(slots, LANES).astype(BF16)
    total = total + dot(weight_hi, returned) + dot(weight_lo, returned)
    out[...] = total.astype(BF16)
    wait_bytes(h_recv.at[pl.ds(1, n_ep - 1)], h_sem.at[0])


def body(n_ep, n_tp, *args):
    (
        tokens, old_state, first_gain, query_weight, key_weight, value_weight, outgate_weight, lowrank_weight,
        decay_weight, decay_bias, head_gain, output_weight, second_gain, expert_gate, expert_up, expert_down,
        shared_gate, shared_up, shared_down, route_ids, route_weights,
    ) = args
    seqs, width = tokens.shape
    dk = old_state.shape[1]
    heads = decay_weight.shape[1] // dk
    chunks = CHUNKS
    blocks = width // LANES
    operands = [
        tokens, old_state, first_gain.reshape(blocks, LANES), query_weight, key_weight, value_weight, outgate_weight,
        lowrank_weight.T, decay_weight, decay_bias.reshape(-1, LANES), head_gain.reshape(1, -1), output_weight,
        second_gain.reshape(blocks, LANES), expert_gate.swapaxes(1, 2), expert_up.swapaxes(1, 2), expert_down,
        shared_gate.T, shared_up.T, shared_down, route_ids.T, route_weights.T,
    ]
    rows = 2 * n_ep // chunks
    vmem = lambda shape, dtype=BF16: pltpu.VMEM(shape, dtype)
    dma = pltpu.SemaphoreType.DMA
    scratch = [vmem(x.shape, x.dtype) for x in operands]
    scratch += [
        vmem((seqs, width)),
        vmem((seqs, LANES)),
        vmem((heads, seqs, 2 * dk)),
        vmem((n_tp - 1, seqs, 2 * dk)),
        vmem((n_tp, 2 * seqs, LANES)),
        vmem((n_tp, 2 * seqs, LANES)),
        vmem((seqs, LANES)),
        vmem((n_tp, seqs, LANES)),
        vmem((seqs, width)),
        vmem((n_tp, seqs, LANES)),
        vmem((n_tp - 1, seqs, LANES)),
        vmem((n_ep, 2, LANES)),
        vmem((n_ep, 2, LANES)),
        vmem((chunks, rows, LANES)),
        vmem((chunks, n_tp, rows, LANES)),
        vmem((rows, width)),
        vmem((chunks, n_tp, rows, LANES)),
        vmem((chunks, n_tp - 1, rows, LANES)),
        vmem((n_ep, 2, LANES)),
        vmem((n_ep, 2, LANES)),
        dma((len(operands),)),
        dma((2,)),
        dma((2,)),
        dma((2,)),
        dma((2,)),
        dma((1 + chunks,)),
        dma((chunks, 2)),
        dma((chunks, 2)),
        dma((2,)),
        pltpu.SemaphoreType.REGULAR((4,)),
    ]
    return pl.pallas_call(
        functools.partial(kernel, (n_ep, n_tp, heads, chunks)),
        out_shape=(
            pltpu.VMEM((seqs, LANES), BF16),
            pltpu.VMEM(old_state.shape, BF16),
        ),
        in_specs=[pl.BlockSpec(memory_space=pltpu.HBM)] * len(operands),
        out_specs=(pl.BlockSpec(memory_space=pltpu.VMEM), pl.BlockSpec(memory_space=pltpu.VMEM)),
        scratch_shapes=scratch,
        compiler_params=pltpu.CompilerParams(
            collective_id=0, has_side_effects=True
        ),
    )(*operands)


def solution(mesh):
    return jax.shard_map(
        functools.partial(body, mesh.shape["ep"], mesh.shape["tp"]),
        mesh=mesh,
        in_specs=(
            P("ep", None),
            P("ep", None, "tp"),
            P(),
            P("tp", None),
            P("tp", None),
            P(None, "tp"),
            P(None, "tp"),
            P(),
            P(),
            P(),
            P("tp"),
            P("tp", None),
            P(),
            P("ep", None, "tp"),
            P("ep", None, "tp"),
            P("ep", "tp", None),
            P(None, "tp"),
            P(None, "tp"),
            P("tp", None),
            P("ep", None),
            P("ep", None),
        ),
        out_specs=(P("ep", "tp"), P("ep", None, "tp")),
        check_vma=False,
    )
```

```python
import functools

import jax
import jax.numpy as jnp
from jax import lax
from jax.experimental import pallas as pl
from jax.experimental.pallas import tpu as pltpu
from jax.sharding import PartitionSpec as P

EPSILON = 1e-06
LANES = 128
CHUNKS = 4
MESH = pl.DeviceIdType.MESH
F32 = jnp.float32
BF16 = jnp.bfloat16


def dot(left, right):
    return jnp.dot(left, right, preferred_element_type=F32)


def dot_t(left, right):
    return lax.dot_general(left, right, (((1,), (1,)), ((), ())), preferred_element_type=F32)


def silu(x):
    return x / (1.0 + jnp.exp(-x))


def kernel(
    sizes,
    tokens_h, state_h, gain1_h, wq_h, wk_h, wv_h, wo_h, wl_h, wd_h, bias_h, hgain_h, wout_h, gain2_h,
    eg_h, eu_h, ed_h, sg_h, su_h, sd_h, ids_h, rw_h,
    out, newstate,
    tokens, state, gain1, wq, wk, wv, wo, wl, wd, bias, hgain, wout, gain2, eg, eu, ed, sg, su, sd, ids, rw,
    normed, own_normed, a_send, a_recv, b_send, b_recv, c_send, c_recv, n2, s_send, s_recv,
    d_send, d_recv, e_send, e_recv, xn, g_send, g_recv, h_send, h_recv,
    in_sem, a_sem, b_sem, c_sem, s_sem, d_sem, e_sem, g_sem, h_sem, z_sem,
):
    n_ep, n_tp, heads, chunks = sizes
    seqs, width = tokens.shape
    dk, vc = state.shape[1], state.shape[2]
    blocks = width // LANES
    per_head = n_tp // heads
    head_width = vc * per_head
    slots = n_ep * 2
    n_chunk = n_ep // chunks
    rows = n_chunk * 2
    p = lax.axis_index("ep")
    t = lax.axis_index("tp")
    head = t // per_head
    own_cols = pl.ds(pl.multiple_of(t * LANES, LANES), LANES)

    def offset_of(i):
        odd = lax.rem(i, 2)
        return odd * ((i + 1) // 2) + (1 - odd) * lax.rem(n_ep - i // 2, n_ep)

    def ep_peer(i):
        return lax.rem(p + offset_of(i), n_ep)

    def wait_bytes(region, sem):
        pltpu.make_async_copy(region, region, sem).wait()

    side = 4 if n_tp == 16 else 1
    hops = [0, 1, 2, 1]
    steps = [(dy, dx) for dy in range(side) for dx in range(side)][1:] if side > 1 else range(1, n_tp)
    steps = sorted(steps, key=lambda s: -(hops[s[0]] + hops[s[1]])) if side > 1 else steps

    def partner(s):
        if side == 1:
            return lax.rem(t + s, n_tp)
        return lax.rem(t // side + s[0], side) * side + lax.rem(t + s[1], side)

    tp_partners = [partner(s) for s in steps]

    def to_tp(src_of, dst_of, sems):
        for k, q in enumerate(tp_partners):
            pltpu.make_async_remote_copy(
                src_of(q), dst_of(k), sems.at[0], sems.at[1], device_id=(p, q), device_id_type=MESH
            ).start()

    def unrolled(count, step):
        width_of = next(u for u in (7, 5, 4, 3, 2, 1) if count % u == 0)

        def some(j, carry):
            for u in range(width_of):
                step(j * width_of + u)
            return carry

        lax.fori_loop(0, count // width_of, some, 0)

    pairs = [
        (tokens_h, tokens), (gain1_h, gain1), (wq_h, wq), (wk_h, wk), (wl_h, wl), (wd_h, wd), (bias_h, bias),
        (wv_h, wv), (wo_h, wo), (ids_h, ids), (rw_h, rw), (hgain_h, hgain), (state_h, state), (wout_h, wout),
        (gain2_h, gain2), (sg_h, sg), (su_h, su), (sd_h, sd), (eg_h, eg), (eu_h, eu), (ed_h, ed),
    ]
    loads = {}
    for number, (src, dst) in enumerate(pairs):
        loads[id(dst)] = (src, dst, in_sem.at[number])

    def ready(*refs):
        for ref in refs:
            pltpu.make_async_copy(*loads[id(ref)]).wait()

    barrier = pltpu.get_barrier_semaphore()
    n_z = n_ep // 2
    z, core = p // 2, lax.rem(p, 2)

    def chip(d):
        return lax.rem(z + n_z + d, n_z)

    near = [2 * z + 1 - core] + [2 * chip(d) + c for d in (1, -1) for c in (0, 1)]
    for _, dst in pairs[:2]:
        pltpu.make_async_copy(*loads[id(dst)]).start()
    for q in near:
        pl.semaphore_signal(barrier, inc=1, device_id=(q, t), device_id_type=MESH)
    for q in tp_partners:
        pl.semaphore_signal(barrier, inc=1, device_id=(p, q), device_id_type=MESH)
    for _, dst in pairs[2:12]:
        pltpu.make_async_copy(*loads[id(dst)]).start()

    rounds = []
    while 2 ** len(rounds) < n_z // 2:
        rounds.append(2 ** len(rounds))

    def tell(r):
        if r < len(rounds):
            for d in (rounds[r], -rounds[r]):
                pl.semaphore_signal(z_sem.at[r], inc=1, device_id=(2 * chip(d) + core, t), device_id_type=MESH)

    def hear(r):
        if r < len(rounds):
            pl.semaphore_wait(z_sem.at[r], 2)

    ready(tokens)
    ready(gain1)
    squares = jnp.zeros((seqs, LANES), F32)
    for j in range(blocks):
        x = tokens[:, j * LANES : (j + 1) * LANES].astype(F32)
        squares += x * x
    inverse = lax.rsqrt(jnp.sum(squares, axis=1, keepdims=True) / width + EPSILON)
    gains = gain1[...].astype(F32)
    for j in range(blocks):
        x = tokens[:, j * LANES : (j + 1) * LANES].astype(F32)
        normed[:, j * LANES : (j + 1) * LANES] = (x * inverse * gains[j : j + 1, :]).astype(BF16)
    own_normed[...] = normed[:, own_cols]

    pl.semaphore_wait(barrier, n_tp - 1 + len(near))
    tell(0)

    ready(wq)
    ready(wk)
    query_part = dot(own_normed[...], wq[...]).astype(BF16)
    key_part = dot(own_normed[...], wk[...]).astype(BF16)
    for h in range(heads):
        a_send[h, :, :dk] = query_part[:, h * dk : (h + 1) * dk]
        a_send[h, :, dk:] = key_part[:, h * dk : (h + 1) * dk]

    to_tp(lambda q: a_send.at[q // per_head], lambda k: a_recv.at[k], a_sem)

    for _, dst in pairs[12:]:
        pltpu.make_async_copy(*loads[id(dst)]).start()

    ready(wl)
    ready(wd)
    ready(bias)
    lowrank = dot_t(normed[...], wl[...]).astype(BF16)
    head_cols = pl.ds(pl.multiple_of(head * dk, dk), dk)
    decay_in = dot(lowrank, wd[:, head_cols])
    bias_all = bias[...]
    bias_row = lax.broadcasted_iota(jnp.int32, bias_all.shape, 0)
    bias_cols = [
        jnp.sum(jnp.where(bias_row == head * (dk // LANES) + m, bias_all, 0.0), axis=0, keepdims=True)
        for m in range(dk // LANES)
    ]
    decay_in = decay_in + jnp.concatenate(bias_cols, axis=1)
    log_decay = -(jnp.maximum(-decay_in, 0.0) + jnp.log1p(jnp.exp(-jnp.abs(decay_in)))) / 16.0
    decay = jnp.exp(log_decay)
    ready(wv)
    ready(wo)
    value = dot(normed[...], wv[...]).astype(BF16)
    out_gate = dot(normed[...], wo[...]).astype(BF16)
    ready(hgain)
    gate = hgain[...].astype(F32) * silu(out_gate.astype(F32))

    ready(ids)
    ready(rw)
    row = lax.broadcasted_iota(jnp.int32, (slots, seqs), 0)
    slot = row // 2
    odd = slot % 2
    offset = odd * ((slot + 1) // 2) + (1 - odd) * ((n_ep - slot // 2) % n_ep)
    expert = (p + offset) % n_ep
    route_ids = ids[...]
    route_weights = rw[...]
    named = jnp.zeros((slots, seqs), F32)
    weight = jnp.zeros((slots, seqs), F32)
    for j in range(route_ids.shape[0]):
        hit = route_ids[j : j + 1, :] == expert
        named = named + jnp.where(hit, 1.0, 0.0)
        weight = weight + jnp.where(hit, route_weights[j : j + 1, :], 0.0)
    earlier = (
        lax.broadcasted_iota(jnp.int32, (seqs, seqs), 0) < lax.broadcasted_iota(jnp.int32, (seqs, seqs), 1)
    )
    rank = dot(named.astype(BF16), jnp.where(earlier, 1.0, 0.0).astype(BF16))
    chosen = jnp.where(rank == (row % 2).astype(F32), named, 0.0)
    placing = chosen.astype(BF16)
    weight = jnp.concatenate([weight * chosen, jnp.zeros((slots, LANES - seqs), F32)], axis=1).T[:seqs]
    weight_hi = weight.astype(BF16)
    weight_lo = (weight - weight_hi.astype(F32)).astype(BF16)

    ready(state)
    ready(wout)

    hear(0)
    tell(1)
    hear(1)
    tell(2)
    hear(2)
    tell(3)

    wait_bytes(a_recv, a_sem.at[1])
    total = a_send[head].astype(F32)
    for k in range(n_tp - 1):
        total = total + a_recv[k].astype(F32)
    query = total[:, :dk].astype(BF16)
    key = total[:, dk:].astype(BF16)
    query_f, key_f = query.astype(F32), key.astype(F32)

    decayed = query_f * decay
    decayed_hi = decayed.astype(BF16)
    decayed_lo = (decayed - decayed_hi.astype(F32)).astype(BF16)
    both = jnp.concatenate([decayed_hi, decayed_lo], axis=0)
    row = lax.broadcasted_iota(jnp.int32, (seqs, vc), 0)
    read = jnp.sum(query_f * key_f, axis=1, keepdims=True) * value.astype(F32)
    for b in range(seqs):
        got = dot(both, state[b])
        read = read + jnp.where(row == b, got[:seqs] + got[seqs:], 0.0)
    read = read * dk**-0.5
    own_squares = jnp.sum(read * read, axis=1, keepdims=True)
    mixed = (read * gate).astype(BF16)
    part = dot(mixed, wout[...]).astype(BF16)
    sq_hi = own_squares.astype(BF16).astype(F32)
    sq_lo = (own_squares - sq_hi).astype(BF16).astype(F32)
    first_lanes = lax.broadcasted_iota(jnp.int32, (seqs, LANES), 1)
    carried_squares = jnp.where(first_lanes == 0, sq_hi, jnp.where(first_lanes == 1, sq_lo, 0.0)).astype(BF16)
    for q in range(n_tp):
        b_send[q, :seqs, :] = part[:, q * LANES : (q + 1) * LANES]
        b_send[q, seqs:, :] = carried_squares
    to_tp(lambda q: b_send.at[q], lambda k: b_recv.at[t], b_sem)
    b_recv[t] = b_send[t]

    padded = jnp.concatenate(
        [
            key_f,
            decay.astype(BF16).astype(F32),
            (decay - decay.astype(BF16).astype(F32)),
            jnp.zeros((LANES - 3 * seqs, dk), F32),
        ],
        axis=0,
    )
    columns = padded.T.astype(BF16)
    value_rows = jnp.concatenate([value.astype(F32), jnp.zeros((LANES - seqs, vc), F32)], axis=0)
    wide_row = lax.broadcasted_iota(jnp.int32, (LANES, vc), 0)
    ready(gain2)
    gains = gain2[...].astype(F32)

    def update(b, carry):
        right = jnp.concatenate(
            [
                jnp.where(wide_row == b, value_rows, 0.0),
                jnp.where((wide_row == seqs + b) | (wide_row == 2 * seqs + b), 1.0, 0.0),
            ],
            axis=1,
        ).astype(BF16)
        made = dot(columns, right)
        newstate[b] = (made[:, vc:] * state[b].astype(F32) + made[:, :vc]).astype(BF16)
        return carry

    lax.fori_loop(0, seqs, update, 0)

    wait_bytes(b_recv.at[pl.ds(0, n_tp - 1)], b_sem.at[1])
    second = tokens[:, own_cols].astype(F32)
    for h in range(heads):
        parts = jnp.zeros((seqs, LANES), F32)
        sums = jnp.zeros((seqs, LANES), F32)
        for q in range(h * per_head, (h + 1) * per_head):
            got = b_recv[q].astype(F32)
            parts = parts + got[:seqs]
            sums = sums + got[seqs:]
        scale = lax.rsqrt(jnp.sum(sums, axis=1, keepdims=True) / head_width + EPSILON)
        second = second + scale * parts
    second = second.astype(BF16)
    c_send[...] = second

    d_send[...] = dot(placing, second).reshape(n_ep, 2, LANES).astype(BF16)

    hear(3)

    def dispatch(step):
        i = n_ep - 1 - step
        pltpu.make_async_remote_copy(
            d_send.at[i], d_recv.at[i], d_sem.at[0], d_sem.at[1 + i // n_chunk],
            device_id=(ep_peer(i), t), device_id_type=MESH,
        ).start()

    unrolled(n_ep - 1, dispatch)
    to_tp(lambda q: c_send, lambda k: c_recv.at[t], c_sem)
    c_recv[t] = second
    d_recv[0] = d_send[0]

    def normalise(pieces, result, count):
        squares = jnp.zeros((count, LANES), F32)
        for j in range(blocks):
            x = pieces(j).astype(F32)
            squares = squares + x * x
        inverse = lax.rsqrt(jnp.sum(squares, axis=1, keepdims=True) / width + EPSILON)
        for j in range(blocks):
            x = pieces(j).astype(F32)
            result[:, j * LANES : (j + 1) * LANES] = (x * inverse * gains[j : j + 1, :]).astype(BF16)

    def shared():
        wait_bytes(c_recv.at[pl.ds(0, n_tp - 1)], c_sem.at[1])
        normalise(lambda j: c_recv[j], n2, seqs)
        ready(sg)
        ready(su)
        ready(sd)
        hidden = (silu(dot_t(n2[...], sg[...])) * dot_t(n2[...], su[...])).astype(BF16)
        down = dot(hidden, sd[...]).astype(BF16)
        for q in range(n_tp):
            s_send[q] = down[:, q * LANES : (q + 1) * LANES]
        to_tp(lambda q: s_send.at[q], lambda k: s_recv.at[k], s_sem)

    def gather(c):
        first = 1 if c == 0 else c * n_chunk
        wait_bytes(d_recv.at[pl.ds(first, (c + 1) * n_chunk - first)], d_sem.at[1 + c])
        block = d_recv[c * n_chunk : (c + 1) * n_chunk].astype(F32).reshape(rows, LANES).astype(BF16)
        e_send[c] = block
        to_tp(lambda q: e_send.at[c], lambda k: e_recv.at[c, t], e_sem.at[c])
        e_recv[c, t] = block

    def experts(c):
        if c == 0:
            ready(eg, eu, ed)
        wait_bytes(e_recv.at[c, pl.ds(0, n_tp - 1)], e_sem.at[c, 1])
        normalise(lambda j: e_recv[c, j], xn, rows)
        hidden = (silu(dot_t(xn[...], eg[0])) * dot_t(xn[...], eu[0])).astype(BF16)
        down = dot(hidden, ed[0]).astype(BF16)
        for q in range(n_tp):
            g_send[c, q] = down[:, q * LANES : (q + 1) * LANES]
        to_tp(lambda q: g_send.at[c, q], lambda k: g_recv.at[c, k], g_sem.at[c])

    def give_back(c):
        wait_bytes(g_recv.at[c], g_sem.at[c, 1])
        total = g_send[c, t].astype(F32)
        for k in range(n_tp - 1):
            total = total + g_recv[c, k].astype(F32)
        h_send[c * n_chunk : (c + 1) * n_chunk] = total.reshape(n_chunk, 2, LANES).astype(BF16)
        first = 1 if c == 0 else c * n_chunk

        def step(s):
            i = (c + 1) * n_chunk - 1 - s
            back = lax.rem(p + n_ep - offset_of(i), n_ep)
            pltpu.make_async_remote_copy(
                h_send.at[i], h_recv.at[i], h_sem.at[0], h_sem.at[1],
                device_id=(back, t), device_id_type=MESH,
            ).start()

        unrolled((c + 1) * n_chunk - first, step)
        if c == 0:
            h_recv[0] = h_send[0]

    gather(0)
    shared()
    gather(1)
    gather(2)
    experts(0)
    gather(3)
    experts(1)
    experts(2)
    experts(3)
    for c in range(chunks):
        give_back(c)

    wait_bytes(s_recv, s_sem.at[1])
    total = s_send[t].astype(F32)
    for k in range(n_tp - 1):
        total = total + s_recv[k].astype(F32)
    total = total + c_send[...].astype(F32)
    wait_bytes(a_recv, a_sem.at[0])
    wait_bytes(b_recv.at[pl.ds(0, n_tp - 1)], b_sem.at[0])
    wait_bytes(c_recv.at[pl.ds(0, n_tp - 1)], c_sem.at[0])
    wait_bytes(s_recv, s_sem.at[0])
    wait_bytes(d_recv.at[pl.ds(1, n_ep - 1)], d_sem.at[0])
    for c in range(chunks):
        wait_bytes(e_recv.at[c, pl.ds(0, n_tp - 1)], e_sem.at[c, 0])
        wait_bytes(g_recv.at[c], g_sem.at[c, 0])

    wait_bytes(h_recv.at[pl.ds(1, n_ep - 1)], h_sem.at[1])
    returned = h_recv[...].astype(F32).reshape(slots, LANES).astype(BF16)
    total = total + dot(weight_hi, returned) + dot(weight_lo, returned)
    out[...] = total.astype(BF16)
    wait_bytes(h_recv.at[pl.ds(1, n_ep - 1)], h_sem.at[0])


def body(n_ep, n_tp, *args):
    (
        tokens, old_state, first_gain, query_weight, key_weight, value_weight, outgate_weight, lowrank_weight,
        decay_weight, decay_bias, head_gain, output_weight, second_gain, expert_gate, expert_up, expert_down,
        shared_gate, shared_up, shared_down, route_ids, route_weights,
    ) = args
    seqs, width = tokens.shape
    dk = old_state.shape[1]
    heads = decay_weight.shape[1] // dk
    chunks = CHUNKS
    blocks = width // LANES
    operands = [
        tokens, old_state, first_gain.reshape(blocks, LANES), query_weight, key_weight, value_weight, outgate_weight,
        lowrank_weight.T, decay_weight, decay_bias.reshape(-1, LANES), head_gain.reshape(1, -1), output_weight,
        second_gain.reshape(blocks, LANES), expert_gate.swapaxes(1, 2), expert_up.swapaxes(1, 2), expert_down,
        shared_gate.T, shared_up.T, shared_down, route_ids.T, route_weights.T,
    ]
    rows = 2 * n_ep // chunks
    vmem = lambda shape, dtype=BF16: pltpu.VMEM(shape, dtype)
    dma = pltpu.SemaphoreType.DMA
    scratch = [vmem(x.shape, x.dtype) for x in operands]
    scratch += [
        vmem((seqs, width)),
        vmem((seqs, LANES)),
        vmem((heads, seqs, 2 * dk)),
        vmem((n_tp - 1, seqs, 2 * dk)),
        vmem((n_tp, 2 * seqs, LANES)),
        vmem((n_tp, 2 * seqs, LANES)),
        vmem((seqs, LANES)),
        vmem((n_tp, seqs, LANES)),
        vmem((seqs, width)),
        vmem((n_tp, seqs, LANES)),
        vmem((n_tp - 1, seqs, LANES)),
        vmem((n_ep, 2, LANES)),
        vmem((n_ep, 2, LANES)),
        vmem((chunks, rows, LANES)),
        vmem((chunks, n_tp, rows, LANES)),
        vmem((rows, width)),
        vmem((chunks, n_tp, rows, LANES)),
        vmem((chunks, n_tp - 1, rows, LANES)),
        vmem((n_ep, 2, LANES)),
        vmem((n_ep, 2, LANES)),
        dma((len(operands),)),
        dma((2,)),
        dma((2,)),
        dma((2,)),
        dma((2,)),
        dma((1 + chunks,)),
        dma((chunks, 2)),
        dma((chunks, 2)),
        dma((2,)),
        pltpu.SemaphoreType.REGULAR((4,)),
    ]
    return pl.pallas_call(
        functools.partial(kernel, (n_ep, n_tp, heads, chunks)),
        out_shape=(
            pltpu.VMEM((seqs, LANES), BF16),
            pltpu.VMEM(old_state.shape, BF16),
        ),
        in_specs=[pl.BlockSpec(memory_space=pltpu.HBM)] * len(operands),
        out_specs=(pl.BlockSpec(memory_space=pltpu.VMEM), pl.BlockSpec(memory_space=pltpu.VMEM)),
        scratch_shapes=scratch,
        compiler_params=pltpu.CompilerParams(
            collective_id=0, has_side_effects=True
        ),
    )(*operands)


def solution(mesh):
    return jax.shard_map(
        functools.partial(body, mesh.shape["ep"], mesh.shape["tp"]),
        mesh=mesh,
        in_specs=(
            P("ep", None),
            P("ep", None, "tp"),
            P(),
            P("tp", None),
            P("tp", None),
            P(None, "tp"),
            P(None, "tp"),
            P(),
            P(),
            P(),
            P("tp"),
            P("tp", None),
            P(),
            P("ep", None, "tp"),
            P("ep", None, "tp"),
            P("ep", "tp", None),
            P(None, "tp"),
            P(None, "tp"),
            P("tp", None),
            P("ep", None),
            P("ep", None),
        ),
        out_specs=(P("ep", "tp"), P("ep", None, "tp")),
        check_vma=False,
    )
```

```python
import functools

import jax
import jax.numpy as jnp
from jax import lax
from jax.experimental import pallas as pl
from jax.experimental.pallas import tpu as pltpu
from jax.sharding import PartitionSpec as P

EPSILON = 1e-06
LANES = 128
GATHERED = (8, 8, 16, 16, 8, 8)
TAKEN = (16, 16, 16, 8, 8)
MESH = pl.DeviceIdType.MESH
F32 = jnp.float32
BF16 = jnp.bfloat16


def dot(left, right):
    return jnp.dot(left, right, preferred_element_type=F32)


def dot_t(left, right):
    return lax.dot_general(left, right, (((1,), (1,)), ((), ())), preferred_element_type=F32)


def silu(x):
    return x / (1.0 + jnp.exp(-x))


def kernel(
    sizes,
    tokens_h, state_h, gain1_h, wq_h, wk_h, wv_h, wo_h, wl_h, wd_h, bias_h, hgain_h, wout_h, gain2_h,
    eg_h, eu_h, ed_h, sg_h, su_h, sd_h, ids_h, rw_h,
    out, newstate,
    tokens, state, gain1, wq, wk, wv, wo, wl, wd, bias, hgain, wout, gain2, eg, eu, ed, sg, su, sd, ids, rw,
    normed, own_normed, a_send, a_recv, q_send, q_recv, b_send, b_recv, c_send, c_recv, s_send, s_recv,
    d_send, d_recv, e_send, e_recv, g_send, g_recv, h_send, h_recv,
    in_sem, a_sem, q_sem, b_sem, c_sem, s_sem, d_sem, e_sem, g_sem, h_sem, z_sem,
):
    n_ep, n_tp, heads, counts, taken = sizes
    starts = [sum(counts[:c]) for c in range(len(counts))]
    taken_starts = [sum(taken[:c]) for c in range(len(taken))]
    seqs, width = tokens.shape
    dk, vc = state.shape[1], state.shape[2]
    blocks = width // LANES
    per_head = n_tp // heads
    head_width = vc * per_head
    slots = n_ep * 2
    p = lax.axis_index("ep")
    t = lax.axis_index("tp")
    head = t // per_head
    own_cols = pl.ds(pl.multiple_of(t * LANES, LANES), LANES)

    def offset_of(i):
        odd = lax.rem(i, 2)
        return odd * ((i + 1) // 2) + (1 - odd) * lax.rem(n_ep - i // 2, n_ep)

    def ep_peer(i):
        return lax.rem(p + offset_of(i), n_ep)

    def wait_bytes(region, sem):
        pltpu.make_async_copy(region, region, sem).wait()

    side = 4 if n_tp == 16 else 1
    hops = [0, 1, 2, 1]
    steps = [(dy, dx) for dy in range(side) for dx in range(side)][1:] if side > 1 else range(1, n_tp)
    steps = sorted(steps, key=lambda s: -(hops[s[0]] + hops[s[1]])) if side > 1 else steps

    def partner(s):
        if side == 1:
            return lax.rem(t + s, n_tp)
        return lax.rem(t // side + s[0], side) * side + lax.rem(t + s[1], side)

    tp_partners = [partner(s) for s in steps]

    def to_tp(src_of, dst_of, sems):
        for k, q in enumerate(tp_partners):
            pltpu.make_async_remote_copy(
                src_of(q), dst_of(k), sems.at[0], sems.at[1], device_id=(p, q), device_id_type=MESH
            ).start()

    def unrolled(count, step):
        width_of = next(u for u in (7, 5, 4, 3, 2, 1) if count % u == 0)

        def some(j, carry):
            for u in range(width_of):
                step(j * width_of + u)
            return carry

        lax.fori_loop(0, count // width_of, some, 0)

    pairs = [
        (tokens_h, tokens), (gain1_h, gain1), (wq_h, wq), (wk_h, wk), (wl_h, wl), (wd_h, wd), (bias_h, bias),
        (wv_h, wv), (wo_h, wo), (ids_h, ids), (rw_h, rw), (hgain_h, hgain), (state_h, state), (wout_h, wout),
        (gain2_h, gain2), (sg_h, sg), (su_h, su), (sd_h, sd), (eg_h, eg), (eu_h, eu), (ed_h, ed),
    ]
    loads = {}
    for number, (src, dst) in enumerate(pairs):
        loads[id(dst)] = (src, dst, in_sem.at[number])

    def ready(*refs):
        for ref in refs:
            pltpu.make_async_copy(*loads[id(ref)]).wait()

    barrier = pltpu.get_barrier_semaphore()
    n_z = n_ep // 2
    z, core = p // 2, lax.rem(p, 2)

    def chip(d):
        return lax.rem(z + n_z + d, n_z)

    near = [2 * z + 1 - core] + [2 * chip(d) + c for d in (1, -1) for c in (0, 1)]
    for _, dst in pairs[:2]:
        pltpu.make_async_copy(*loads[id(dst)]).start()
    for q in near:
        pl.semaphore_signal(barrier, inc=1, device_id=(q, t), device_id_type=MESH)
    for q in tp_partners:
        pl.semaphore_signal(barrier, inc=1, device_id=(p, q), device_id_type=MESH)
    for _, dst in pairs[2:4]:
        pltpu.make_async_copy(*loads[id(dst)]).start()

    rounds = []
    while 2 ** len(rounds) < n_z // 2:
        rounds.append(2 ** len(rounds))

    def tell(r):
        if r < len(rounds):
            for d in (rounds[r], -rounds[r]):
                pl.semaphore_signal(z_sem.at[r], inc=1, device_id=(2 * chip(d) + core, t), device_id_type=MESH)

    def hear(r):
        if r < len(rounds):
            pl.semaphore_wait(z_sem.at[r], 2)

    ready(tokens)
    ready(gain1)
    squares = jnp.zeros((seqs, LANES), F32)
    for j in range(blocks):
        x = tokens[:, j * LANES : (j + 1) * LANES].astype(F32)
        squares += x * x
    inverse = lax.rsqrt(jnp.sum(squares, axis=1, keepdims=True) / width + EPSILON)
    gains = gain1[...].astype(F32)
    for j in range(blocks):
        x = tokens[:, j * LANES : (j + 1) * LANES].astype(F32)
        normed[:, j * LANES : (j + 1) * LANES] = (x * inverse * gains[j : j + 1, :]).astype(BF16)
    own_normed[...] = normed[:, own_cols]
    for _, dst in pairs[4:12]:
        pltpu.make_async_copy(*loads[id(dst)]).start()

    ready(wq)
    ready(wk)
    query_part = dot(own_normed[...], wq[...]).astype(BF16)
    key_part = dot(own_normed[...], wk[...]).astype(BF16)
    for h in range(heads):
        a_send[h, :, :dk] = query_part[:, h * dk : (h + 1) * dk]
        a_send[h, :, dk:] = key_part[:, h * dk : (h + 1) * dk]

    pl.semaphore_wait(barrier, n_tp - 1 + len(near))
    tell(0)
    to_tp(lambda q: a_send.at[q // per_head], lambda k: a_recv.at[k], a_sem)

    for _, dst in pairs[12:]:
        pltpu.make_async_copy(*loads[id(dst)]).start()

    ready(wl)
    ready(wd)
    ready(bias)
    lowrank = dot_t(normed[...], wl[...]).astype(BF16)
    head_cols = pl.ds(pl.multiple_of(head * dk, dk), dk)
    decay_in = dot(lowrank, wd[:, head_cols])
    bias_all = bias[...]
    bias_row = lax.broadcasted_iota(jnp.int32, bias_all.shape, 0)
    bias_cols = [
        jnp.sum(jnp.where(bias_row == head * (dk // LANES) + m, bias_all, 0.0), axis=0, keepdims=True)
        for m in range(dk // LANES)
    ]
    decay_in = decay_in + jnp.concatenate(bias_cols, axis=1)
    log_decay = -(jnp.maximum(-decay_in, 0.0) + jnp.log1p(jnp.exp(-jnp.abs(decay_in)))) / 16.0
    decay = jnp.exp(log_decay)
    ready(wv)
    ready(wo)
    value = dot(normed[...], wv[...]).astype(BF16)
    out_gate = dot(normed[...], wo[...]).astype(BF16)
    ready(hgain)
    gate = hgain[...].astype(F32) * silu(out_gate.astype(F32))

    ready(ids)
    ready(rw)
    row = lax.broadcasted_iota(jnp.int32, (slots, seqs), 0)
    slot = row // 2
    odd = slot % 2
    offset = odd * ((slot + 1) // 2) + (1 - odd) * ((n_ep - slot // 2) % n_ep)
    expert = (p + offset) % n_ep
    route_ids = ids[...]
    route_weights = rw[...]
    named = jnp.zeros((slots, seqs), F32)
    weight = jnp.zeros((slots, seqs), F32)
    for j in range(route_ids.shape[0]):
        hit = route_ids[j : j + 1, :] == expert
        named = named + jnp.where(hit, 1.0, 0.0)
        weight = weight + jnp.where(hit, route_weights[j : j + 1, :], 0.0)
    earlier = (
        lax.broadcasted_iota(jnp.int32, (seqs, seqs), 0) < lax.broadcasted_iota(jnp.int32, (seqs, seqs), 1)
    )
    rank = dot(named.astype(BF16), jnp.where(earlier, 1.0, 0.0).astype(BF16))
    chosen = jnp.where(rank == (row % 2).astype(F32), named, 0.0)
    placing = chosen.astype(BF16)
    weight = jnp.concatenate([weight * chosen, jnp.zeros((slots, LANES - seqs), F32)], axis=1).T[:seqs]
    weight_hi = weight.astype(BF16)
    weight_lo = (weight - weight_hi.astype(F32)).astype(BF16)

    ready(state)
    ready(wout)

    hear(0)
    tell(1)
    hear(1)
    tell(2)
    hear(2)
    tell(3)

    wait_bytes(a_recv, a_sem.at[1])
    total = a_send[head].astype(F32)
    for k in range(n_tp - 1):
        total = total + a_recv[k].astype(F32)
    query = total[:, :dk].astype(BF16)
    key = total[:, dk:].astype(BF16)
    query_f, key_f = query.astype(F32), key.astype(F32)

    decayed = query_f * decay
    decayed_hi = decayed.astype(BF16)
    decayed_lo = (decayed - decayed_hi.astype(F32)).astype(BF16)
    both = jnp.concatenate([decayed_hi, decayed_lo], axis=0)
    row = lax.broadcasted_iota(jnp.int32, (seqs, vc), 0)
    read = jnp.sum(query_f * key_f, axis=1, keepdims=True) * value.astype(F32)
    for b in range(seqs):
        got = dot(both, state[b])
        read = read + jnp.where(row == b, got[:seqs] + got[seqs:], 0.0)
    read = read * dk**-0.5
    mixed = (read * gate).astype(BF16)
    part = dot(mixed, wout[...]).astype(BF16)
    for q in range(n_tp):
        b_send[q] = part[:, q * LANES : (q + 1) * LANES]
    to_tp(lambda q: b_send.at[q], lambda k: b_recv.at[t], b_sem)
    squared = read * read
    squared_hi = squared.astype(BF16)
    squared_lo = (squared - squared_hi.astype(F32)).astype(BF16)
    ones = jnp.ones((2 * seqs, vc), BF16)
    own_squares = dot_t(ones, jnp.concatenate([squared_hi, jnp.zeros((LANES - seqs, vc), BF16)], axis=0))
    own_squares += dot_t(ones, jnp.concatenate([squared_lo, jnp.zeros((LANES - seqs, vc), BF16)], axis=0))
    square_row = lax.broadcasted_iota(jnp.int32, own_squares.shape, 0)
    square_hi = own_squares.astype(BF16).astype(F32)
    q_send[...] = jnp.where(square_row == 0, square_hi, own_squares - square_hi)[:2].astype(BF16)
    to_tp(lambda q: q_send, lambda k: q_recv.at[t], q_sem)
    q_recv[t] = q_send[...]
    b_recv[t] = b_send[t]

    padded = jnp.concatenate(
        [
            key_f,
            decay.astype(BF16).astype(F32),
            (decay - decay.astype(BF16).astype(F32)),
            jnp.zeros((LANES - 3 * seqs, dk), F32),
        ],
        axis=0,
    )
    columns = padded.T.astype(BF16)
    value_rows = jnp.concatenate([value.astype(F32), jnp.zeros((LANES - seqs, vc), F32)], axis=0)
    wide_row = lax.broadcasted_iota(jnp.int32, (LANES, vc), 0)
    ready(gain2)
    gains = gain2[...].astype(F32)

    def update(b, carry):
        right = jnp.concatenate(
            [
                jnp.where(wide_row == b, value_rows, 0.0),
                jnp.where((wide_row == seqs + b) | (wide_row == 2 * seqs + b), 1.0, 0.0),
            ],
            axis=1,
        ).astype(BF16)
        made = dot(columns, right)
        newstate[b] = (made[:, vc:] * state[b].astype(F32) + made[:, :vc]).astype(BF16)
        return carry

    lax.fori_loop(0, seqs, update, 0)

    wait_bytes(q_recv.at[pl.ds(0, n_tp - 1)], q_sem.at[1])
    head_sums = []
    for h in range(heads):
        sums = jnp.zeros((2, LANES), F32)
        for q in range(h * per_head, (h + 1) * per_head):
            sums = sums + q_recv[q].astype(F32)
        head_sums.append(jnp.sum(sums, axis=0, keepdims=True))
    head_sums = jnp.concatenate(head_sums + [jnp.zeros((LANES - heads, LANES), F32)], axis=0).T[:seqs]
    scales = lax.rsqrt(head_sums / head_width + EPSILON)
    wait_bytes(b_recv.at[pl.ds(0, n_tp - 1)], b_sem.at[1])
    second = tokens[:, own_cols].astype(F32)
    for h in range(heads):
        parts = jnp.zeros((seqs, LANES), F32)
        for q in range(h * per_head, (h + 1) * per_head):
            parts = parts + b_recv[q].astype(F32)
        second = second + scales[:, h : h + 1] * parts
    second = second.astype(BF16)
    c_send[...] = second

    d_send[...] = dot(placing, second).reshape(n_ep, 2, LANES).astype(BF16)

    hear(3)

    def dispatch(c, step):
        i = starts[c] + counts[c] - 1 - step
        pltpu.make_async_remote_copy(
            d_send.at[i], d_recv.at[i], d_sem.at[0], d_sem.at[1 + c],
            device_id=(ep_peer(i), t), device_id_type=MESH,
        ).start()

    for c in range(len(counts) - 1, -1, -1):
        unrolled(counts[c] - (c == 0), functools.partial(dispatch, c))
    to_tp(lambda q: c_send, lambda k: c_recv.at[t], c_sem)
    c_recv[t] = second
    d_recv[0] = d_send[0]

    def scale_of(pieces, count):
        squares = jnp.zeros((count, LANES), F32)
        for piece in pieces:
            x = piece.astype(F32)
            squares = squares + x * x
        return lax.rsqrt(jnp.sum(squares, axis=1, keepdims=True) / width + EPSILON)

    ready(eg, eu, sg, su)
    for j in range(blocks):
        cols = slice(j * LANES, (j + 1) * LANES)
        for w in (eg.at[0], eu.at[0], sg, su):
            w[:, cols] = (w[:, cols].astype(F32) * gains[j : j + 1, :]).astype(BF16)

    def hidden_of(pieces, count, gate_w, up_w):
        x = jnp.concatenate(pieces, axis=1)
        scale = scale_of(pieces, count)
        return (silu(dot_t(x, gate_w) * scale) * (dot_t(x, up_w) * scale)).astype(BF16)

    def shared():
        wait_bytes(c_recv.at[pl.ds(0, n_tp - 1)], c_sem.at[1])
        ready(sd)
        hidden = hidden_of([c_recv[j] for j in range(blocks)], seqs, sg[...], su[...])
        down = dot(hidden, sd[...]).astype(BF16)
        for q in range(n_tp):
            s_send[q] = down[:, q * LANES : (q + 1) * LANES]
        to_tp(lambda q: s_send.at[q], lambda k: s_recv.at[k], s_sem)

    def sources(c):
        return pl.ds(max(starts[c], 1), counts[c] - (c == 0))

    def gather(c):
        rows = pl.ds(2 * starts[c], 2 * counts[c])
        wait_bytes(d_recv.at[sources(c)], d_sem.at[1 + c])
        block = d_recv[starts[c] : starts[c] + counts[c]].astype(F32).reshape(2 * counts[c], LANES).astype(BF16)
        e_send[rows] = block
        to_tp(lambda q: e_send.at[rows], lambda k: e_recv.at[t, rows], e_sem.at[c])
        e_recv[t, rows] = block

    def experts(c):
        if c == 0:
            ready(ed)
        rows = pl.ds(2 * taken_starts[c], 2 * taken[c])
        for m in range(len(counts)):
            if taken_starts[c] <= starts[m] < taken_starts[c] + taken[c]:
                some = pl.ds(2 * starts[m], 2 * counts[m])
                wait_bytes(e_recv.at[pl.ds(0, n_tp - 1), some], e_sem.at[m, 1])
        hidden = hidden_of([e_recv[j, rows] for j in range(blocks)], 2 * taken[c], eg[0], eu[0])
        down = dot(hidden, ed[0]).astype(BF16)
        for q in range(n_tp):
            g_send[q, rows] = down[:, q * LANES : (q + 1) * LANES]
        to_tp(lambda q: g_send.at[q, rows], lambda k: g_recv.at[k, rows], g_sem.at[c])

    def give_back(c):
        first, count = taken_starts[c], taken[c]
        rows = pl.ds(2 * first, 2 * count)
        wait_bytes(g_recv.at[pl.ds(0, n_tp - 1), rows], g_sem.at[c, 1])
        total = g_send[t, rows].astype(F32)
        for k in range(n_tp - 1):
            total = total + g_recv[k, rows].astype(F32)
        h_send[first : first + count] = total.reshape(count, 2, LANES).astype(BF16)

        def step(s):
            i = first + count - 1 - s
            back = lax.rem(p + n_ep - offset_of(i), n_ep)
            pltpu.make_async_remote_copy(
                h_send.at[i], h_recv.at[i], h_sem.at[0], h_sem.at[1],
                device_id=(back, t), device_id_type=MESH,
            ).start()

        unrolled(count - (c == 0), step)
        if c == 0:
            h_recv[0] = h_send[0]

    for c in range(len(counts)):
        gather(c)
    for c in range(len(taken)):
        experts(c)
    for c in range(len(taken)):
        give_back(c)
    shared()

    wait_bytes(s_recv, s_sem.at[1])
    total = s_send[t].astype(F32)
    for k in range(n_tp - 1):
        total = total + s_recv[k].astype(F32)
    total = total + c_send[...].astype(F32)
    wait_bytes(a_recv, a_sem.at[0])
    wait_bytes(q_recv.at[pl.ds(0, n_tp - 1)], q_sem.at[0])
    wait_bytes(b_recv.at[pl.ds(0, n_tp - 1)], b_sem.at[0])
    wait_bytes(c_recv.at[pl.ds(0, n_tp - 1)], c_sem.at[0])
    wait_bytes(s_recv, s_sem.at[0])
    wait_bytes(d_recv.at[pl.ds(1, n_ep - 1)], d_sem.at[0])
    for c in range(len(counts)):
        wait_bytes(e_recv.at[pl.ds(0, n_tp - 1), pl.ds(2 * starts[c], 2 * counts[c])], e_sem.at[c, 0])
    for c in range(len(taken)):
        wait_bytes(g_recv.at[pl.ds(0, n_tp - 1), pl.ds(2 * taken_starts[c], 2 * taken[c])], g_sem.at[c, 0])

    wait_bytes(h_recv.at[pl.ds(1, n_ep - 1)], h_sem.at[1])
    returned = h_recv[...].astype(F32).reshape(slots, LANES).astype(BF16)
    total = total + dot(weight_hi, returned) + dot(weight_lo, returned)
    out[...] = total.astype(BF16)
    wait_bytes(h_recv.at[pl.ds(1, n_ep - 1)], h_sem.at[0])


def finish(x, state_in, out, state_out, sem):
    copies = [pltpu.make_async_copy(state_in, state_out, sem.at[0]), pltpu.make_async_copy(x, out, sem.at[1])]
    for copy in copies:
        copy.start()
    for copy in copies:
        copy.wait()


def body(n_ep, n_tp, *args):
    (
        tokens, old_state, first_gain, query_weight, key_weight, value_weight, outgate_weight, lowrank_weight,
        decay_weight, decay_bias, head_gain, output_weight, second_gain, expert_gate, expert_up, expert_down,
        shared_gate, shared_up, shared_down, route_ids, route_weights,
    ) = args
    seqs, width = tokens.shape
    dk = old_state.shape[1]
    heads = decay_weight.shape[1] // dk
    counts = tuple(n_ep * x // 64 for x in GATHERED)
    taken = tuple(n_ep * x // 64 for x in TAKEN)
    blocks = width // LANES
    operands = [
        tokens, old_state, first_gain.reshape(blocks, LANES), query_weight, key_weight, value_weight, outgate_weight,
        lowrank_weight.T, decay_weight, decay_bias.reshape(-1, LANES), head_gain.reshape(1, -1), output_weight,
        second_gain.reshape(blocks, LANES), expert_gate.swapaxes(1, 2), expert_up.swapaxes(1, 2), expert_down,
        shared_gate.T, shared_up.T, shared_down, route_ids.T, route_weights.T,
    ]
    rows = 2 * n_ep
    vmem = lambda shape, dtype=BF16: pltpu.VMEM(shape, dtype)
    dma = pltpu.SemaphoreType.DMA
    scratch = [vmem(x.shape, x.dtype) for x in operands]
    scratch += [
        vmem((seqs, width)),
        vmem((seqs, LANES)),
        vmem((heads, seqs, 2 * dk)),
        vmem((n_tp - 1, seqs, 2 * dk)),
        vmem((2, LANES)),
        vmem((n_tp, 2, LANES)),
        vmem((n_tp, seqs, LANES)),
        vmem((n_tp, seqs, LANES)),
        vmem((seqs, LANES)),
        vmem((n_tp, seqs, LANES)),
        vmem((n_tp, seqs, LANES)),
        vmem((n_tp - 1, seqs, LANES)),
        vmem((n_ep, 2, LANES)),
        vmem((n_ep, 2, LANES)),
        vmem((rows, LANES)),
        vmem((n_tp, rows, LANES)),
        vmem((n_tp, rows, LANES)),
        vmem((n_tp - 1, rows, LANES)),
        vmem((n_ep, 2, LANES)),
        vmem((n_ep, 2, LANES)),
        dma((len(operands),)),
        dma((2,)),
        dma((2,)),
        dma((2,)),
        dma((2,)),
        dma((2,)),
        dma((1 + len(counts),)),
        dma((len(counts), 2)),
        dma((len(taken), 2)),
        dma((2,)),
        pltpu.SemaphoreType.REGULAR((4,)),
    ]
    results = pl.pallas_call(
        functools.partial(kernel, (n_ep, n_tp, heads, counts, taken)),
        out_shape=(
            pltpu.VMEM((seqs, LANES), BF16),
            pltpu.VMEM(old_state.shape, BF16),
        ),
        in_specs=[pl.BlockSpec(memory_space=pltpu.HBM)] * len(operands),
        out_specs=(pl.BlockSpec(memory_space=pltpu.VMEM), pl.BlockSpec(memory_space=pltpu.VMEM)),
        scratch_shapes=scratch,
        compiler_params=pltpu.CompilerParams(
            collective_id=0, has_side_effects=True
        ),
    )(*operands)
    results = [pltpu.with_memory_space_constraint(x, pltpu.VMEM) for x in results]
    return pl.pallas_call(
        finish,
        out_shape=(
            jax.ShapeDtypeStruct((seqs, LANES), BF16),
            jax.ShapeDtypeStruct(old_state.shape, BF16),
        ),
        in_specs=[pl.BlockSpec(memory_space=pl.ANY), pl.BlockSpec(memory_space=pl.ANY)],
        out_specs=(pl.BlockSpec(memory_space=pltpu.HBM), pl.BlockSpec(memory_space=pltpu.HBM)),
        scratch_shapes=[dma((2,))],
    )(*results)


def solution(mesh):
    return jax.shard_map(
        functools.partial(body, mesh.shape["ep"], mesh.shape["tp"]),
        mesh=mesh,
        in_specs=(
            P("ep", None),
            P("ep", None, "tp"),
            P(),
            P("tp", None),
            P("tp", None),
            P(None, "tp"),
            P(None, "tp"),
            P(),
            P(),
            P(),
            P("tp"),
            P("tp", None),
            P(),
            P("ep", None, "tp"),
            P("ep", None, "tp"),
            P("ep", "tp", None),
            P(None, "tp"),
            P(None, "tp"),
            P("tp", None),
            P("ep", None),
            P("ep", None),
        ),
        out_specs=(P("ep", "tp"), P("ep", None, "tp")),
        check_vma=False,
    )
```

```python
import functools

import jax
import jax.numpy as jnp
from jax import lax
from jax.experimental import pallas as pl
from jax.experimental.pallas import tpu as pltpu
from jax.sharding import PartitionSpec as P

EPSILON = 1e-06
LANES = 128
GATHERED = (8, 8, 16, 16, 8, 8)
TAKEN = (16, 16, 16, 8, 8)
MESH = pl.DeviceIdType.MESH
F32 = jnp.float32
BF16 = jnp.bfloat16


def dot(left, right):
    return jnp.dot(left, right, preferred_element_type=F32)


def dot_t(left, right):
    return lax.dot_general(left, right, (((1,), (1,)), ((), ())), preferred_element_type=F32)


def silu(x):
    return x / (1.0 + jnp.exp(-x))


def kernel(
    sizes,
    tokens_h, state_h, gain1_h, wq_h, wk_h, wv_h, wo_h, wl_h, wd_h, bias_h, hgain_h, wout_h, gain2_h,
    eg_h, eu_h, ed_h, sg_h, su_h, sd_h, ids_h, rw_h,
    out, newstate,
    tokens, state, gain1, wq, wk, wv, wo, wl, wd, bias, hgain, wout, gain2, eg, eu, ed, sg, su, sd, ids, rw,
    normed, own_normed, a_send, a_recv, q_send, q_recv, b_send, b_recv, c_send, c_recv, s_send, s_recv,
    d_send, d_recv, e_send, e_recv, g_send, g_recv, h_send, h_recv,
    in_sem, a_sem, q_sem, b_sem, c_sem, s_sem, d_sem, e_sem, g_sem, h_sem, z_sem,
):
    n_ep, n_tp, heads, counts, taken = sizes
    starts = [sum(counts[:c]) for c in range(len(counts))]
    taken_starts = [sum(taken[:c]) for c in range(len(taken))]
    seqs, width = tokens.shape
    dk, vc = state.shape[1], state.shape[2]
    blocks = width // LANES
    per_head = n_tp // heads
    head_width = vc * per_head
    slots = n_ep * 2
    p = lax.axis_index("ep")
    t = lax.axis_index("tp")
    head = t // per_head
    own_cols = pl.ds(pl.multiple_of(t * LANES, LANES), LANES)

    def offset_of(i):
        odd = lax.rem(i, 2)
        return odd * ((i + 1) // 2) + (1 - odd) * lax.rem(n_ep - i // 2, n_ep)

    def ep_peer(i):
        return lax.rem(p + offset_of(i), n_ep)

    def wait_bytes(region, sem):
        pltpu.make_async_copy(region, region, sem).wait()

    side = 4 if n_tp == 16 else 1
    hops = [0, 1, 2, 1]
    steps = [(dy, dx) for dy in range(side) for dx in range(side)][1:] if side > 1 else range(1, n_tp)
    steps = sorted(steps, key=lambda s: -(hops[s[0]] + hops[s[1]])) if side > 1 else steps

    def partner(s):
        if side == 1:
            return lax.rem(t + s, n_tp)
        return lax.rem(t // side + s[0], side) * side + lax.rem(t + s[1], side)

    tp_partners = [partner(s) for s in steps]

    def to_tp(src_of, dst_of, sems):
        for k, q in enumerate(tp_partners):
            pltpu.make_async_remote_copy(
                src_of(q), dst_of(k), sems.at[0], sems.at[1], device_id=(p, q), device_id_type=MESH
            ).start()

    def unrolled(count, step):
        width_of = next(u for u in (7, 5, 4, 3, 2, 1) if count % u == 0)

        def some(j, carry):
            for u in range(width_of):
                step(j * width_of + u)
            return carry

        lax.fori_loop(0, count // width_of, some, 0)

    pairs = [
        (tokens_h, tokens), (gain1_h, gain1), (wq_h, wq), (wk_h, wk), (wl_h, wl), (wd_h, wd), (bias_h, bias),
        (wv_h, wv), (wo_h, wo), (ids_h, ids), (rw_h, rw), (hgain_h, hgain), (state_h, state), (wout_h, wout),
        (gain2_h, gain2), (sg_h, sg), (su_h, su), (sd_h, sd), (eg_h, eg), (eu_h, eu), (ed_h, ed),
    ]
    loads = {}
    for number, (src, dst) in enumerate(pairs):
        loads[id(dst)] = (src, dst, in_sem.at[number])

    def ready(*refs):
        for ref in refs:
            pltpu.make_async_copy(*loads[id(ref)]).wait()

    barrier = pltpu.get_barrier_semaphore()
    n_z = n_ep // 2
    z, core = p // 2, lax.rem(p, 2)

    def chip(d):
        return lax.rem(z + n_z + d, n_z)

    near = [2 * z + 1 - core] + [2 * chip(d) + c for d in (1, -1) for c in (0, 1)]
    for _, dst in pairs[:2]:
        pltpu.make_async_copy(*loads[id(dst)]).start()
    for q in near:
        pl.semaphore_signal(barrier, inc=1, device_id=(q, t), device_id_type=MESH)
    for q in tp_partners:
        pl.semaphore_signal(barrier, inc=1, device_id=(p, q), device_id_type=MESH)
    for _, dst in pairs[2:4]:
        pltpu.make_async_copy(*loads[id(dst)]).start()

    rounds = []
    while 2 ** len(rounds) < n_z // 2:
        rounds.append(2 ** len(rounds))

    def tell(r):
        if r < len(rounds):
            for d in (rounds[r], -rounds[r]):
                pl.semaphore_signal(z_sem.at[r], inc=1, device_id=(2 * chip(d) + core, t), device_id_type=MESH)

    def hear(r):
        if r < len(rounds):
            pl.semaphore_wait(z_sem.at[r], 2)

    ready(tokens)
    ready(gain1)
    squares = jnp.zeros((seqs, LANES), F32)
    for j in range(blocks):
        x = tokens[:, j * LANES : (j + 1) * LANES].astype(F32)
        squares += x * x
    inverse = lax.rsqrt(jnp.sum(squares, axis=1, keepdims=True) / width + EPSILON)
    gains = gain1[...].astype(F32)
    for j in range(blocks):
        x = tokens[:, j * LANES : (j + 1) * LANES].astype(F32)
        normed[:, j * LANES : (j + 1) * LANES] = (x * inverse * gains[j : j + 1, :]).astype(BF16)
    own_normed[...] = normed[:, own_cols]
    for _, dst in pairs[4:12]:
        pltpu.make_async_copy(*loads[id(dst)]).start()

    ready(wq)
    ready(wk)
    query_part = dot(own_normed[...], wq[...]).astype(BF16)
    key_part = dot(own_normed[...], wk[...]).astype(BF16)
    for h in range(heads):
        a_send[h, :, :dk] = query_part[:, h * dk : (h + 1) * dk]
        a_send[h, :, dk:] = key_part[:, h * dk : (h + 1) * dk]

    pl.semaphore_wait(barrier, n_tp - 1 + len(near))
    tell(0)
    to_tp(lambda q: a_send.at[q // per_head], lambda k: a_recv.at[k], a_sem)

    for _, dst in pairs[12:]:
        pltpu.make_async_copy(*loads[id(dst)]).start()

    ready(wl)
    ready(wd)
    ready(bias)
    lowrank = dot_t(normed[...], wl[...]).astype(BF16)
    head_cols = pl.ds(pl.multiple_of(head * dk, dk), dk)
    decay_in = dot(lowrank, wd[:, head_cols])
    bias_all = bias[...]
    bias_row = lax.broadcasted_iota(jnp.int32, bias_all.shape, 0)
    bias_cols = [
        jnp.sum(jnp.where(bias_row == head * (dk // LANES) + m, bias_all, 0.0), axis=0, keepdims=True)
        for m in range(dk // LANES)
    ]
    decay_in = decay_in + jnp.concatenate(bias_cols, axis=1)
    log_decay = -(jnp.maximum(-decay_in, 0.0) + jnp.log1p(jnp.exp(-jnp.abs(decay_in)))) / 16.0
    decay = jnp.exp(log_decay)
    ready(wv)
    ready(wo)
    value = dot(normed[...], wv[...]).astype(BF16)
    out_gate = dot(normed[...], wo[...]).astype(BF16)
    ready(hgain)
    gate = hgain[...].astype(F32) * silu(out_gate.astype(F32))

    ready(ids)
    ready(rw)
    row = lax.broadcasted_iota(jnp.int32, (slots, seqs), 0)
    slot = row // 2
    odd = slot % 2
    offset = odd * ((slot + 1) // 2) + (1 - odd) * ((n_ep - slot // 2) % n_ep)
    expert = (p + offset) % n_ep
    route_ids = ids[...]
    route_weights = rw[...]
    named = jnp.zeros((slots, seqs), F32)
    weight = jnp.zeros((slots, seqs), F32)
    for j in range(route_ids.shape[0]):
        hit = route_ids[j : j + 1, :] == expert
        named = named + jnp.where(hit, 1.0, 0.0)
        weight = weight + jnp.where(hit, route_weights[j : j + 1, :], 0.0)
    earlier = (
        lax.broadcasted_iota(jnp.int32, (seqs, seqs), 0) < lax.broadcasted_iota(jnp.int32, (seqs, seqs), 1)
    )
    rank = dot(named.astype(BF16), jnp.where(earlier, 1.0, 0.0).astype(BF16))
    chosen = jnp.where(rank == (row % 2).astype(F32), named, 0.0)
    placing = chosen.astype(BF16)
    weight = jnp.concatenate([weight * chosen, jnp.zeros((slots, LANES - seqs), F32)], axis=1).T[:seqs]
    weight_hi = weight.astype(BF16)
    weight_lo = (weight - weight_hi.astype(F32)).astype(BF16)

    ready(state)
    ready(wout)

    hear(0)
    tell(1)
    hear(1)
    tell(2)
    hear(2)
    tell(3)

    wait_bytes(a_recv, a_sem.at[1])
    total = a_send[head].astype(F32)
    for k in range(n_tp - 1):
        total = total + a_recv[k].astype(F32)
    query = total[:, :dk].astype(BF16)
    key = total[:, dk:].astype(BF16)
    query_f, key_f = query.astype(F32), key.astype(F32)

    decayed = query_f * decay
    decayed_hi = decayed.astype(BF16)
    decayed_lo = (decayed - decayed_hi.astype(F32)).astype(BF16)
    both = jnp.concatenate([decayed_hi, decayed_lo], axis=0)
    row = lax.broadcasted_iota(jnp.int32, (seqs, vc), 0)
    read = jnp.sum(query_f * key_f, axis=1, keepdims=True) * value.astype(F32)
    for b in range(seqs):
        got = dot(both, state[b])
        read = read + jnp.where(row == b, got[:seqs] + got[seqs:], 0.0)
    read = read * dk**-0.5
    mixed = (read * gate).astype(BF16)
    part = dot(mixed, wout[...]).astype(BF16)
    for q in range(n_tp):
        b_send[q] = part[:, q * LANES : (q + 1) * LANES]
    to_tp(lambda q: b_send.at[q], lambda k: b_recv.at[t], b_sem)
    squared = read * read
    squared_hi = squared.astype(BF16)
    squared_lo = (squared - squared_hi.astype(F32)).astype(BF16)
    ones = jnp.ones((2 * seqs, vc), BF16)
    own_squares = dot_t(ones, jnp.concatenate([squared_hi, jnp.zeros((LANES - seqs, vc), BF16)], axis=0))
    own_squares += dot_t(ones, jnp.concatenate([squared_lo, jnp.zeros((LANES - seqs, vc), BF16)], axis=0))
    square_row = lax.broadcasted_iota(jnp.int32, own_squares.shape, 0)
    square_hi = own_squares.astype(BF16).astype(F32)
    q_send[...] = jnp.where(square_row == 0, square_hi, own_squares - square_hi)[:2].astype(BF16)
    to_tp(lambda q: q_send, lambda k: q_recv.at[t], q_sem)
    q_recv[t] = q_send[...]
    b_recv[t] = b_send[t]

    padded = jnp.concatenate(
        [
            key_f,
            decay.astype(BF16).astype(F32),
            (decay - decay.astype(BF16).astype(F32)),
            jnp.zeros((LANES - 3 * seqs, dk), F32),
        ],
        axis=0,
    )
    columns = padded.T.astype(BF16)
    value_rows = jnp.concatenate([value.astype(F32), jnp.zeros((LANES - seqs, vc), F32)], axis=0)
    wide_row = lax.broadcasted_iota(jnp.int32, (LANES, vc), 0)
    ready(gain2)
    gains = gain2[...].astype(F32)

    def update(b, carry):
        right = jnp.concatenate(
            [
                jnp.where(wide_row == b, value_rows, 0.0),
                jnp.where((wide_row == seqs + b) | (wide_row == 2 * seqs + b), 1.0, 0.0),
            ],
            axis=1,
        ).astype(BF16)
        made = dot(columns, right)
        newstate[b] = (made[:, vc:] * state[b].astype(F32) + made[:, :vc]).astype(BF16)
        return carry

    lax.fori_loop(0, seqs, update, 0)

    wait_bytes(q_recv.at[pl.ds(0, n_tp - 1)], q_sem.at[1])
    head_sums = []
    for h in range(heads):
        sums = jnp.zeros((2, LANES), F32)
        for q in range(h * per_head, (h + 1) * per_head):
            sums = sums + q_recv[q].astype(F32)
        head_sums.append(jnp.sum(sums, axis=0, keepdims=True))
    head_sums = jnp.concatenate(head_sums + [jnp.zeros((LANES - heads, LANES), F32)], axis=0).T[:seqs]
    scales = lax.rsqrt(head_sums / head_width + EPSILON)
    wait_bytes(b_recv.at[pl.ds(0, n_tp - 1)], b_sem.at[1])
    second = tokens[:, own_cols].astype(F32)
    for h in range(heads):
        parts = jnp.zeros((seqs, LANES), F32)
        for q in range(h * per_head, (h + 1) * per_head):
            parts = parts + b_recv[q].astype(F32)
        second = second + scales[:, h : h + 1] * parts
    second = second.astype(BF16)
    c_send[...] = second

    d_send[...] = dot(placing, second).reshape(n_ep, 2, LANES).astype(BF16)

    hear(3)

    def dispatch(c, step):
        i = starts[c] + counts[c] - 1 - step
        pltpu.make_async_remote_copy(
            d_send.at[i], d_recv.at[i], d_sem.at[0], d_sem.at[1 + c],
            device_id=(ep_peer(i), t), device_id_type=MESH,
        ).start()

    for c in range(len(counts) - 1, -1, -1):
        unrolled(counts[c] - (c == 0), functools.partial(dispatch, c))
    to_tp(lambda q: c_send, lambda k: c_recv.at[t], c_sem)
    c_recv[t] = second
    d_recv[0] = d_send[0]

    def scale_of(pieces, count):
        squares = jnp.zeros((count, LANES), F32)
        for piece in pieces:
            x = piece.astype(F32)
            squares = squares + x * x
        return lax.rsqrt(jnp.sum(squares, axis=1, keepdims=True) / width + EPSILON)

    ready(eg, eu, sg, su)
    for j in range(blocks):
        cols = slice(j * LANES, (j + 1) * LANES)
        for w in (eg.at[0], eu.at[0], sg, su):
            w[:, cols] = (w[:, cols].astype(F32) * gains[j : j + 1, :]).astype(BF16)

    def hidden_of(pieces, count, gate_w, up_w):
        x = jnp.concatenate(pieces, axis=1)
        scale = scale_of(pieces, count)
        return (silu(dot_t(x, gate_w) * scale) * (dot_t(x, up_w) * scale)).astype(BF16)

    def shared():
        wait_bytes(c_recv.at[pl.ds(0, n_tp - 1)], c_sem.at[1])
        ready(sd)
        hidden = hidden_of([c_recv[j] for j in range(blocks)], seqs, sg[...], su[...])
        down = dot(hidden, sd[...]).astype(BF16)
        for q in range(n_tp):
            s_send[q] = down[:, q * LANES : (q + 1) * LANES]
        to_tp(lambda q: s_send.at[q], lambda k: s_recv.at[k], s_sem)

    def sources(c):
        return pl.ds(max(starts[c], 1), counts[c] - (c == 0))

    def gather(c):
        rows = pl.ds(2 * starts[c], 2 * counts[c])
        wait_bytes(d_recv.at[sources(c)], d_sem.at[1 + c])
        block = d_recv[starts[c] : starts[c] + counts[c]].astype(F32).reshape(2 * counts[c], LANES).astype(BF16)
        e_send[rows] = block
        to_tp(lambda q: e_send.at[rows], lambda k: e_recv.at[t, rows], e_sem.at[c])
        e_recv[t, rows] = block

    def experts(c):
        if c == 0:
            ready(ed)
        rows = pl.ds(2 * taken_starts[c], 2 * taken[c])
        for m in range(len(counts)):
            if taken_starts[c] <= starts[m] < taken_starts[c] + taken[c]:
                some = pl.ds(2 * starts[m], 2 * counts[m])
                wait_bytes(e_recv.at[pl.ds(0, n_tp - 1), some], e_sem.at[m, 1])
        hidden = hidden_of([e_recv[j, rows] for j in range(blocks)], 2 * taken[c], eg[0], eu[0])
        down = dot(hidden, ed[0]).astype(BF16)
        for q in range(n_tp):
            g_send[q, rows] = down[:, q * LANES : (q + 1) * LANES]
        to_tp(lambda q: g_send.at[q, rows], lambda k: g_recv.at[k, rows], g_sem.at[c])

    def give_back(c):
        first, count = taken_starts[c], taken[c]
        rows = pl.ds(2 * first, 2 * count)
        wait_bytes(g_recv.at[pl.ds(0, n_tp - 1), rows], g_sem.at[c, 1])
        total = g_send[t, rows].astype(F32)
        for k in range(n_tp - 1):
            total = total + g_recv[k, rows].astype(F32)
        h_send[first : first + count] = total.reshape(count, 2, LANES).astype(BF16)

        def step(s):
            i = first + count - 1 - s
            back = lax.rem(p + n_ep - offset_of(i), n_ep)
            pltpu.make_async_remote_copy(
                h_send.at[i], h_recv.at[i], h_sem.at[0], h_sem.at[1],
                device_id=(back, t), device_id_type=MESH,
            ).start()

        unrolled(count - (c == 0), step)
        if c == 0:
            h_recv[0] = h_send[0]

    for c in range(len(counts)):
        gather(c)
    for c in range(len(taken)):
        experts(c)
    shared()
    for c in range(len(taken)):
        give_back(c)

    wait_bytes(s_recv, s_sem.at[1])
    total = s_send[t].astype(F32)
    for k in range(n_tp - 1):
        total = total + s_recv[k].astype(F32)
    total = total + c_send[...].astype(F32)
    wait_bytes(a_recv, a_sem.at[0])
    wait_bytes(q_recv.at[pl.ds(0, n_tp - 1)], q_sem.at[0])
    wait_bytes(b_recv.at[pl.ds(0, n_tp - 1)], b_sem.at[0])
    wait_bytes(c_recv.at[pl.ds(0, n_tp - 1)], c_sem.at[0])
    wait_bytes(s_recv, s_sem.at[0])
    wait_bytes(d_recv.at[pl.ds(1, n_ep - 1)], d_sem.at[0])
    for c in range(len(counts)):
        wait_bytes(e_recv.at[pl.ds(0, n_tp - 1), pl.ds(2 * starts[c], 2 * counts[c])], e_sem.at[c, 0])
    for c in range(len(taken)):
        wait_bytes(g_recv.at[pl.ds(0, n_tp - 1), pl.ds(2 * taken_starts[c], 2 * taken[c])], g_sem.at[c, 0])

    wait_bytes(h_recv.at[pl.ds(1, n_ep - 1)], h_sem.at[1])
    returned = h_recv[...].astype(F32).reshape(slots, LANES).astype(BF16)
    total = total + dot(weight_hi, returned) + dot(weight_lo, returned)
    out[...] = total.astype(BF16)
    wait_bytes(h_recv.at[pl.ds(1, n_ep - 1)], h_sem.at[0])


def finish(x, state_in, out, state_out, sem):
    copies = [pltpu.make_async_copy(state_in, state_out, sem.at[0]), pltpu.make_async_copy(x, out, sem.at[1])]
    for copy in copies:
        copy.start()
    for copy in copies:
        copy.wait()


def body(n_ep, n_tp, *args):
    (
        tokens, old_state, first_gain, query_weight, key_weight, value_weight, outgate_weight, lowrank_weight,
        decay_weight, decay_bias, head_gain, output_weight, second_gain, expert_gate, expert_up, expert_down,
        shared_gate, shared_up, shared_down, route_ids, route_weights,
    ) = args
    seqs, width = tokens.shape
    dk = old_state.shape[1]
    heads = decay_weight.shape[1] // dk
    counts = tuple(n_ep * x // 64 for x in GATHERED)
    taken = tuple(n_ep * x // 64 for x in TAKEN)
    blocks = width // LANES
    operands = [
        tokens, old_state, first_gain.reshape(blocks, LANES), query_weight, key_weight, value_weight, outgate_weight,
        lowrank_weight.T, decay_weight, decay_bias.reshape(-1, LANES), head_gain.reshape(1, -1), output_weight,
        second_gain.reshape(blocks, LANES), expert_gate.swapaxes(1, 2), expert_up.swapaxes(1, 2), expert_down,
        shared_gate.T, shared_up.T, shared_down, route_ids.T, route_weights.T,
    ]
    rows = 2 * n_ep
    vmem = lambda shape, dtype=BF16: pltpu.VMEM(shape, dtype)
    dma = pltpu.SemaphoreType.DMA
    scratch = [vmem(x.shape, x.dtype) for x in operands]
    scratch += [
        vmem((seqs, width)),
        vmem((seqs, LANES)),
        vmem((heads, seqs, 2 * dk)),
        vmem((n_tp - 1, seqs, 2 * dk)),
        vmem((2, LANES)),
        vmem((n_tp, 2, LANES)),
        vmem((n_tp, seqs, LANES)),
        vmem((n_tp, seqs, LANES)),
        vmem((seqs, LANES)),
        vmem((n_tp, seqs, LANES)),
        vmem((n_tp, seqs, LANES)),
        vmem((n_tp - 1, seqs, LANES)),
        vmem((n_ep, 2, LANES)),
        vmem((n_ep, 2, LANES)),
        vmem((rows, LANES)),
        vmem((n_tp, rows, LANES)),
        vmem((n_tp, rows, LANES)),
        vmem((n_tp - 1, rows, LANES)),
        vmem((n_ep, 2, LANES)),
        vmem((n_ep, 2, LANES)),
        dma((len(operands),)),
        dma((2,)),
        dma((2,)),
        dma((2,)),
        dma((2,)),
        dma((2,)),
        dma((1 + len(counts),)),
        dma((len(counts), 2)),
        dma((len(taken), 2)),
        dma((2,)),
        pltpu.SemaphoreType.REGULAR((4,)),
    ]
    results = pl.pallas_call(
        functools.partial(kernel, (n_ep, n_tp, heads, counts, taken)),
        out_shape=(
            pltpu.VMEM((seqs, LANES), BF16),
            pltpu.VMEM(old_state.shape, BF16),
        ),
        in_specs=[pl.BlockSpec(memory_space=pltpu.HBM)] * len(operands),
        out_specs=(pl.BlockSpec(memory_space=pltpu.VMEM), pl.BlockSpec(memory_space=pltpu.VMEM)),
        scratch_shapes=scratch,
        compiler_params=pltpu.CompilerParams(
            collective_id=0, has_side_effects=True
        ),
    )(*operands)
    results = [pltpu.with_memory_space_constraint(x, pltpu.VMEM) for x in results]
    return pl.pallas_call(
        finish,
        out_shape=(
            jax.ShapeDtypeStruct((seqs, LANES), BF16),
            jax.ShapeDtypeStruct(old_state.shape, BF16),
        ),
        in_specs=[pl.BlockSpec(memory_space=pl.ANY), pl.BlockSpec(memory_space=pl.ANY)],
        out_specs=(pl.BlockSpec(memory_space=pltpu.HBM), pl.BlockSpec(memory_space=pltpu.HBM)),
        scratch_shapes=[dma((2,))],
    )(*results)


def solution(mesh):
    return jax.shard_map(
        functools.partial(body, mesh.shape["ep"], mesh.shape["tp"]),
        mesh=mesh,
        in_specs=(
            P("ep", None),
            P("ep", None, "tp"),
            P(),
            P("tp", None),
            P("tp", None),
            P(None, "tp"),
            P(None, "tp"),
            P(),
            P(),
            P(),
            P("tp"),
            P("tp", None),
            P(),
            P("ep", None, "tp"),
            P("ep", None, "tp"),
            P("ep", "tp", None),
            P(None, "tp"),
            P(None, "tp"),
            P("tp", None),
            P("ep", None),
            P("ep", None),
        ),
        out_specs=(P("ep", "tp"), P("ep", None, "tp")),
        check_vma=False,
    )
```
